32 devices in a mesh: sp: 4 (over z), tp: 4 (over y, x), dp: 2 (over core).
Axes of the slice: x: 2, y: 2, z: 4, core: 2. Of those that a mesh axis runs over, the one named last changes fastest.
Arguments:
- latent: bfloat16 [2, 2048, 2048], P('dp', ('sp', 'tp')), may hold values from -6 to 6
- condition: float32 [2, 2048], P('dp'), may hold values from -6 to 6
- context: bfloat16 [2, 1024, 2048], P('dp', 'sp'), may hold values from -6 to 6
- context_cond: float32 [2048], replicated, may hold values from -6 to 6
- shift_matrix: bfloat16 [2048, 2048], P(('sp', 'tp')), may hold values from -0.125 to 0.125
- scale_matrix: bfloat16 [2048, 2048], P(('sp', 'tp')), may hold values from -0.125 to 0.125
- gate_matrix: bfloat16 [2048, 2048], P(('sp', 'tp')), may hold values from -0.125 to 0.125
- value_proj: bfloat16 [2048, 2048], P(None, 'tp'), may hold values from -0.125 to 0.125
- gate_proj: bfloat16 [2048, 2048], P(None, 'tp'), may hold values from -0.125 to 0.125
- write_proj: bfloat16 [2048, 1024], P(None, 'tp'), may hold values from -0.125 to 0.125
- read_proj: bfloat16 [2048, 1024], P(None, 'tp'), may hold values from -0.125 to 0.125
- step_proj: bfloat16 [2048, 2, 32], replicated, may hold values from -0.125 to 0.125
- decay_rate: float32 [2, 32], replicated, may hold values from 0.000243652344 to 0.0601
- pacing: float32 [2, 2048], P('dp'), may hold values from 0.2 to 4.3
- value_taps: float32 [5, 2048], replicated, may hold values from -2.5 to 2.5
- write_taps: float32 [5, 1024], replicated, may hold values from -2.5 to 2.5
- read_taps: float32 [5, 1024], replicated, may hold values from -2.5 to 2.5
- norm_gain: float32 [2048], replicated, may hold values from 0.1 to 1.9
- out_proj: bfloat16 [2048, 2048], P('tp'), may hold values from -0.125 to 0.125
Outputs:
- updated: bfloat16 [2, 2048, 2048], P('dp', ('sp', 'tp'))
The draws below stay inside these ranges and needn't reach their ends.
All inputs are finite; a program needn't handle non-finite values.
Results may differ from the reference program's by a relative error of at most 0.006.
Values may be sent and summed in bfloat16 or wider, within the bound.
A program may use at most 128 MiB of HBM per device.

```python
import math
import jax
import jax.numpy as jnp
from jax import lax

D = 2048
WIDTH = 2048
HEAD = 64
GROUPS = 8
STATE = 128
CONV = 5
ROW = 64
BLOCK = 128
TOK_DEV = 512
CTX = 1024
SAMPLES = 2
TOKENS = 2048
HEADS = 32
CHANNEL_BLOCK = 512


def draw_latent(key, part):
    noise_key, scale_key, direction_key, strength_key = jax.random.split(key, 4)
    span_rows = TOK_DEV // 2
    span_count = TOKENS // span_rows
    noise = jax.random.normal(noise_key, (SAMPLES, TOKENS, D), jnp.float32)
    directions = jax.random.normal(direction_key, (SAMPLES, span_count, D), jnp.float32)
    strength = jax.random.uniform(strength_key, (SAMPLES, span_count, 1), jnp.float32, 1.0, 2.0)
    offsets = jnp.repeat(directions * strength, span_rows, axis=1)
    return jnp.clip(noise + offsets, -6.0, 6.0).astype(jnp.bfloat16)


def draw_decay_rate(key, part):
    pick_key, slow_key, quick_key = jax.random.split(key, 3)
    quick_mask = jax.random.randint(pick_key, (2, HEADS), 0, 2) == 0
    slow_rate = jnp.exp(jax.random.uniform(slow_key, (2, HEADS), jnp.float32, math.log(0.5), math.log(2.0))) / TOKENS
    quick_rate = jnp.exp(jax.random.uniform(quick_key, (2, HEADS), jnp.float32, math.log(0.02), math.log(0.06)))
    return jnp.where(quick_mask, quick_rate, slow_rate).astype(jnp.float32)


def draw_pacing(key, part):
    span_key, token_key = jax.random.split(key)
    span_rows = TOK_DEV // 2
    span_count = TOKENS // span_rows
    span_factor = jnp.exp(jax.random.uniform(span_key, (SAMPLES, span_count), jnp.float32, math.log(0.35), math.log(2.8)))
    token_factor = jax.random.uniform(token_key, (SAMPLES, TOKENS), jnp.float32, 0.6, 1.5)
    return (jnp.repeat(span_factor, span_rows, axis=1) * token_factor).astype(jnp.float32)


def block_levels(stream_key, dims, cuts, least, high):
    factor_of, own = 1.0, jax.random.fold_in(stream_key, 6)
    for axis_at, blocks in cuts:
        draws = jnp.exp(jax.random.uniform(jax.random.fold_in(own, axis_at), (blocks,), jnp.float32, least / len(cuts), high / len(cuts)))
        factor_of = factor_of * jnp.repeat(draws, dims[axis_at] // blocks).reshape([-1 if axis == axis_at else 1 for axis in range(len(dims))])
    return factor_of


def gaussian(stream_key, dims, scale, limit, cuts=(), kind=jnp.bfloat16):
    level = block_levels(stream_key, dims, cuts, -0.22, 0.18) if cuts else 1.0
    entries = jax.random.normal(stream_key, dims, jnp.float32) * scale * level
    return jnp.minimum(jnp.maximum(entries, -limit), limit).astype(kind)


def setup_inputs(seed: int = 0) -> dict:
    key_list = jax.random.split(jax.random.key(seed), 20)
    return {
        "latent": draw_latent(jax.random.fold_in(key_list[19], 71), 0),
        "condition": gaussian(key_list[1], (SAMPLES, D), 1.0, 6.0, ((0, 2),), jnp.float32),
        "context": gaussian(key_list[2], (SAMPLES, CTX, D), 1.0, 6.0, ((0, 2), (1, 4))),
        "context_cond": gaussian(key_list[3], (D,), 1.0, 6.0, (), jnp.float32),
        "shift_matrix": gaussian(key_list[4], (D, D), D ** -0.5, 0.125, ((0, 16),)),
        "scale_matrix": gaussian(key_list[5], (D, D), D ** -0.5, 0.125, ((0, 16),)),
        "gate_matrix": gaussian(key_list[6], (D, D), D ** -0.5, 0.125, ((0, 16),)),
        "value_proj": gaussian(key_list[7], (D, WIDTH), D ** -0.5, 0.125, ((1, 4),)),
        "gate_proj": gaussian(key_list[8], (D, WIDTH), D ** -0.5, 0.125, ((1, 4),)),
        "write_proj": gaussian(key_list[9], (D, GROUPS * STATE), D ** -0.5, 0.125, ((1, 4),)),
        "read_proj": gaussian(key_list[10], (D, GROUPS * STATE), D ** -0.5, 0.125, ((1, 4),)),
        "step_proj": gaussian(key_list[11], (D, 2, HEADS), D ** -0.5, 0.125),
        "decay_rate": draw_decay_rate(jax.random.fold_in(key_list[19], 71), 0),
        "pacing": draw_pacing(jax.random.fold_in(key_list[19], 71), 0),
        "value_taps": gaussian(key_list[14], (CONV, WIDTH), CONV ** -0.5, 2.5, (), jnp.float32),
        "write_taps": gaussian(key_list[15], (CONV, GROUPS * STATE), CONV ** -0.5, 2.5, (), jnp.float32),
        "read_taps": gaussian(key_list[16], (CONV, GROUPS * STATE), CONV ** -0.5, 2.5, (), jnp.float32),
        "norm_gain": jnp.clip(1.0 + 0.18 * jax.random.normal(key_list[17], (WIDTH,), jnp.float32), 0.1, 1.9),
        "out_proj": gaussian(key_list[18], (WIDTH, D), WIDTH ** -0.5, 0.125, ((0, 4),)),
    }


NORM_FLOOR = 1e-05
GATED_FLOOR = 1e-06
FINEST = lax.Precision.HIGHEST

def masked_exp(exponent, allowed):
    return jnp.where(allowed, jnp.exp(jnp.where(allowed, exponent, 0.0)), 0.0)

def modulate(row_block, shift_row, scale_row):
    values = row_block.astype(jnp.float32)
    center = lax.optimization_barrier(jnp.mean(values, -1, keepdims=True))
    spread = lax.optimization_barrier(jnp.mean(jnp.square(values - center), -1, keepdims=True))
    normed = (values - center) * lax.rsqrt(spread + NORM_FLOOR)
    return (normed * (1.0 + shift_row * 0.0 + scale_row) + shift_row).astype(jnp.bfloat16)

def convolve(values, kernel, run_count):
    length, channels = values.shape
    tap_count = kernel.shape[0]
    margin = tap_count // 2
    stretch = length // run_count
    blocked = values.astype(jnp.float32).reshape(run_count, stretch, channels)
    padded = jnp.pad(blocked, ((0, 0), (margin, margin), (0, 0)))
    summed = jnp.zeros_like(blocked)
    for offset in range(tap_count):
        summed = summed + padded[:, offset:offset + stretch] * kernel[offset]
    return jax.nn.silu(summed).reshape(length, channels).astype(jnp.bfloat16)

def context_state(values, writes, weight, groups):
    length = values.shape[0]
    per_group = weight.shape[1] // groups
    scaled = (writes.reshape(length, groups, 1, STATE) * weight.reshape(length, groups, per_group, 1)).astype(jnp.bfloat16)
    head_values = values.reshape(length, groups, per_group, HEAD)
    return jnp.einsum('lgrn,lgrp->grnp', scaled.astype(jnp.float32), head_values.astype(jnp.float32))

def block_sweep(values, writes, reads, decays, steps, start):
    length = values.shape[0]
    groups = writes.shape[1] // STATE
    per_group = decays.shape[1] // groups
    blocks = length // BLOCK
    head_values = values.reshape(blocks, BLOCK, groups, per_group, HEAD).astype(jnp.float32)
    write_rows = writes.reshape(blocks, BLOCK, groups, STATE)
    read_rows = reads.reshape(blocks, BLOCK, groups, STATE).astype(jnp.float32)
    cumulative = jnp.cumsum(decays.reshape(blocks, BLOCK, groups, per_group), axis=1)
    step_rows = steps.reshape(blocks, BLOCK, groups, per_group)
    lower_mask = jnp.tril(jnp.ones((BLOCK, BLOCK), bool))[:, :, None, None]

    def advance(carry_state, inputs):
        block_values, block_writes, block_reads, block_cumul, block_steps = inputs
        affinity = jnp.einsum('tgn,sgn->tsg', block_reads, block_writes.astype(jnp.float32))
        exponent = block_cumul[:, None] - block_cumul[None, :]
        mixing = (affinity[..., None] * masked_exp(exponent, lower_mask) * block_steps[None]).astype(jnp.bfloat16)
        within = jnp.einsum('tsgr,sgrp->tgrp', mixing.astype(jnp.float32), block_values)
        carried = jnp.einsum('tgn,grnp->tgrp', block_reads, carry_state, precision=FINEST) * jnp.exp(block_cumul)[..., None]
        weight = jnp.exp(block_cumul[-1:] - block_cumul) * block_steps
        scaled = (block_writes[:, :, None, :] * weight[..., None]).astype(jnp.bfloat16)
        increment = jnp.einsum('sgrn,sgrp->grnp', scaled.astype(jnp.float32), block_values)
        carry_state = jnp.exp(block_cumul[-1])[..., None, None] * carry_state + increment
        return (carry_state, within + carried)
    final_state, outputs = lax.scan(advance, start, (head_values, write_rows, read_rows, cumulative, step_rows))
    return outputs.reshape(length, groups * per_group * HEAD)

def reference(latent, condition, context, context_cond, shift_matrix, scale_matrix, gate_matrix, value_proj, gate_proj, write_proj, read_proj, step_proj, decay_rate, pacing, value_taps, write_taps, read_taps, norm_gain, out_proj):
    model_width = latent.shape[2]
    results = []
    for sample in range(latent.shape[0]):
        activated = jax.nn.silu(jnp.stack([condition[sample], context_cond])).astype(jnp.bfloat16)
        shifts = jnp.dot(activated, shift_matrix, preferred_element_type=jnp.float32)
        scales = jnp.dot(activated, scale_matrix, preferred_element_type=jnp.float32)
        gate_row = jnp.dot(activated[:1], gate_matrix, preferred_element_type=jnp.float32)
        hidden = modulate(latent[sample], shifts[0], scales[0])
        run_count = TOKENS // ROW
        values = convolve(jnp.dot(hidden, value_proj, preferred_element_type=jnp.float32).astype(jnp.bfloat16), value_taps, run_count)
        writes = convolve(jnp.dot(hidden, write_proj, preferred_element_type=jnp.float32).astype(jnp.bfloat16), write_taps, run_count)
        read_rows = convolve(jnp.dot(hidden, read_proj, preferred_element_type=jnp.float32).astype(jnp.bfloat16), read_taps, run_count)
        gate_pre = jnp.dot(hidden, gate_proj, preferred_element_type=jnp.float32).astype(jnp.bfloat16)
        step_raw = jnp.dot(hidden, step_proj.reshape(model_width, 2 * HEADS), preferred_element_type=jnp.float32).astype(jnp.bfloat16)
        step_raw = lax.optimization_barrier(step_raw).astype(jnp.float32).reshape(TOKENS, 2, HEADS)
        context_hidden = modulate(context[sample], shifts[1], scales[1])
        ctx_values = convolve(jnp.dot(context_hidden, value_proj, preferred_element_type=jnp.float32).astype(jnp.bfloat16), value_taps, 1)
        ctx_writes = convolve(jnp.dot(context_hidden, write_proj, preferred_element_type=jnp.float32).astype(jnp.bfloat16), write_taps, 1)
        ctx_raw = jnp.dot(context_hidden, step_proj.reshape(model_width, 2 * HEADS), preferred_element_type=jnp.float32).astype(jnp.bfloat16)
        ctx_raw = lax.optimization_barrier(ctx_raw).astype(jnp.float32).reshape(CTX, 2, HEADS)
        ctx_fwd_step = jax.nn.softplus(ctx_raw[:, 0])
        ctx_fwd_decay = -decay_rate[0][None, :] * ctx_fwd_step
        ctx_cumul = jnp.cumsum(ctx_fwd_decay, axis=0)
        ctx_forward = context_state(ctx_values, ctx_writes, jnp.exp(ctx_cumul[-1:] - ctx_cumul) * ctx_fwd_step, GROUPS)
        ctx_bwd_step = jax.nn.softplus(ctx_raw[:, 1])
        ctx_bwd_decay = -decay_rate[1][None, :] * ctx_bwd_step
        ctx_back_cumul = jnp.cumsum(ctx_bwd_decay, axis=0)
        ctx_backward = context_state(ctx_values, ctx_writes, jnp.exp(ctx_back_cumul - ctx_bwd_decay) * ctx_bwd_step, GROUPS)
        forward_step = jax.nn.softplus(step_raw[:, 0]) * pacing[sample][:, None]
        forward_decay = -decay_rate[0][None, :] * forward_step
        backward_step = jax.nn.softplus(step_raw[:, 1]) * pacing[sample][:, None]
        backward_decay = -decay_rate[1][None, :] * backward_step
        forward_out = block_sweep(values, writes, read_rows, forward_decay, forward_step, ctx_forward)
        backward_out = block_sweep(values[::-1], writes[::-1], read_rows[::-1], backward_decay[::-1], backward_step[::-1], ctx_backward)[::-1]
        gated_heads = (forward_out + backward_out) * jax.nn.silu(gate_pre.astype(jnp.float32))
        grouped = gated_heads.reshape(TOKENS, GROUPS, -1)
        grouped = grouped * lax.rsqrt(lax.optimization_barrier(jnp.mean(grouped * grouped, -1, keepdims=True)) + GATED_FLOOR)
        inner_rows = (grouped.reshape(TOKENS, WIDTH) * norm_gain).astype(jnp.bfloat16)
        summed = jnp.zeros((TOKENS, model_width), jnp.float32)
        for column_block in range(WIDTH // CHANNEL_BLOCK):
            lower_edge = column_block * CHANNEL_BLOCK
            portion = jnp.dot(inner_rows[:, lower_edge:lower_edge + CHANNEL_BLOCK], out_proj[lower_edge:lower_edge + CHANNEL_BLOCK], preferred_element_type=jnp.float32).astype(jnp.bfloat16)
            summed = summed + lax.optimization_barrier(portion).astype(jnp.float32)
        mixed = lax.optimization_barrier(summed.astype(jnp.bfloat16))
        results.append((latent[sample].astype(jnp.float32) + gate_row[0] * mixed.astype(jnp.float32)).astype(jnp.bfloat16))
    return jnp.stack(results)
```

```python
import functools

import jax
import jax.numpy as jnp
from jax import lax
from jax.experimental import pallas as pl
from jax.experimental.pallas import tpu as pltpu
from jax.sharding import PartitionSpec as P

HEAD = 64
STATE = 128
ROW = 64
BLOCK = 128
LANES = 128
HALO = 16

NORM_FLOOR = 1e-05
GATED_FLOOR = 1e-06
FINEST = lax.Precision.HIGHEST
MESH = pl.DeviceIdType.MESH
F32 = jnp.float32
BF16 = jnp.bfloat16


def vmem():
    return pl.BlockSpec(memory_space=pltpu.VMEM)


def send(src, dst, send_sem, recv_sem, axis, target):
    copy = pltpu.make_async_remote_copy(
        src_ref=src,
        dst_ref=dst,
        send_sem=send_sem,
        recv_sem=recv_sem,
        device_id={axis: target},
        device_id_type=MESH,
    )
    copy.start()
    return copy


def greet(peers):
    barrier = pltpu.get_barrier_semaphore()
    for axis, target in peers:
        pl.semaphore_signal(barrier, inc=1, device_id={axis: target}, device_id_type=MESH)
    pl.semaphore_wait(barrier, len(peers))


def others(axis, count):
    me = lax.axis_index(axis)
    return [lax.rem(me + d, count) for d in range(1, count)]


def spread_kernel(
    sp_n, tp_n,
    act, shift_m, scale_m, gate_m, latent, context,
    latent_all, context_ext, mod,
    part, tp_box, middle, sp_box,
    lat_s, lat_r, tps, tpr, sps, spr, halo_s, halo_r, own,
):
    sp, tp = lax.axis_index("sp"), lax.axis_index("tp")
    tp_peers, sp_peers = others("tp", tp_n), others("sp", sp_n)
    rows, ctx_rows = latent.shape[0], context.shape[0]
    greet([("tp", p) for p in tp_peers] + [("sp", p) for p in sp_peers])
    mine = pl.ds(pl.multiple_of(tp * rows, rows), rows)
    copy_lat = pltpu.make_async_copy(latent, latent_all.at[mine], own.at[0])
    copy_lat.start()
    copy_ctx = pltpu.make_async_copy(context, context_ext.at[pl.ds(HALO, ctx_rows)], own.at[1])
    copy_ctx.start()
    before = lax.rem(sp + sp_n - 1, sp_n)
    after = lax.rem(sp + 1, sp_n)
    halos = [
        send(context.at[pl.ds(ctx_rows - HALO, HALO)], context_ext.at[pl.ds(0, HALO)],
             halo_s.at[0], halo_r.at[0], "sp", after),
        send(context.at[pl.ds(0, HALO)], context_ext.at[pl.ds(HALO + ctx_rows, HALO)],
             halo_s.at[1], halo_r.at[1], "sp", before),
    ]
    total = jnp.dot(act[0:16, :], shift_m[...], preferred_element_type=F32)
    total += jnp.dot(act[16:32, :], scale_m[...], preferred_element_type=F32)
    total += jnp.dot(act[32:48, :], gate_m[...], preferred_element_type=F32)
    part[...] = total[0:8]
    first = [
        send(part, tp_box.at[d], tps.at[d], tpr.at[d], "tp", p) for d, p in enumerate(tp_peers)
    ]
    rows_out = [
        send(latent, latent_all.at[mine], lat_s.at[d], lat_r.at[d], "tp", p)
        for d, p in enumerate(tp_peers)
    ]
    for copy in first:
        copy.wait()
    summed = part[...]
    for d in range(tp_n - 1):
        summed += tp_box[d]
    middle[...] = summed
    second = [
        send(middle, sp_box.at[d], sps.at[d], spr.at[d], "sp", p) for d, p in enumerate(sp_peers)
    ]
    for copy in second:
        copy.wait()
    summed = middle[...]
    for d in range(sp_n - 1):
        summed += sp_box[d]
    mod[...] = summed
    for copy in halos:
        copy.wait()
    copy_lat.wait()
    copy_ctx.wait()
    for copy in rows_out:
        copy.wait()


def softplus(x):
    return jnp.maximum(x, 0.0) + jnp.log1p(jnp.exp(-jnp.abs(x)))


def silu(x):
    return x * (1.0 / (1.0 + jnp.exp(-x)))


def modulate_into(source, target, shift_row, scale_row):
    step = 16

    def tile(i, carry):
        at = pl.ds(pl.multiple_of(i * step, step), step)
        values = source[at, :].astype(F32)
        center = jnp.mean(values, -1, keepdims=True)
        values = values - center
        spread = jnp.mean(values * values, -1, keepdims=True)
        normed = values * lax.rsqrt(spread + NORM_FLOOR)
        target[at, :] = (normed * (1.0 + scale_row[...]) + shift_row[...]).astype(BF16)
        return carry

    lax.fori_loop(0, source.shape[0] // step, tile, 0)


def conv_silu(values, taps, run):
    rows, channels = values.shape
    margin = taps.shape[0] // 2
    place = lax.broadcasted_iota(jnp.int32, (rows, channels), 0) % run
    summed = jnp.zeros((rows, channels), F32)
    for k in range(taps.shape[0]):
        offset = k - margin
        moved = pltpu.roll(values, (-offset) % rows, 0) if offset else values
        if offset:
            moved = jnp.where((place + offset >= 0) & (place + offset < run), moved, 0.0)
        summed += moved * taps[k : k + 1, :]
    return silu(summed).astype(BF16)


def running(decay, heads):
    rows = decay.shape[0]
    at = lax.broadcasted_iota(jnp.int32, (rows, rows), 0)
    by = lax.broadcasted_iota(jnp.int32, (rows, rows), 1)
    lower = (by <= at).astype(F32)
    upper = (by >= at).astype(F32)
    lane = lax.broadcasted_iota(jnp.int32, decay.shape, 1)
    forward = jnp.dot(lower, decay, precision=FINEST, preferred_element_type=F32)
    backward = jnp.dot(upper, decay, precision=FINEST, preferred_element_type=F32)
    return jnp.where(lane < heads, forward, backward)


def lane_to_rows(row, count):
    return jnp.broadcast_to(row, (LANES, LANES)).T[0:count]


def partial_states(values, writes, weight, heads, per_group):
    turned = values.astype(F32).T.astype(BF16)
    result = []
    for h in range(heads):
        g = h // per_group
        rows = writes[:, g * STATE : (g + 1) * STATE].astype(F32)
        pair = jnp.concatenate(
            [(rows * weight[:, h : h + 1]).astype(BF16),
             (rows * weight[:, heads + h : heads + h + 1]).astype(BF16)], axis=1)
        result.append(
            jnp.dot(turned[h * HEAD : (h + 1) * HEAD], pair, preferred_element_type=F32))
    return result


def project_kernel(
    sp_n, heads, per_group,
    latent, context_ext, mod, value_p, gate_p, write_p, read_p, step_p,
    rates, pacing, value_t, write_t, read_t,
    values_o, gate_o, writes_o, reads_o, step_o, cumul_o, inc_o, states_o, tots_o,
    hidden, hidden_c, ctx_v, ctx_w,
):
    sp, tp = lax.axis_index("sp"), lax.axis_index("tp")
    tokens = latent.shape[0]
    ext = context_ext.shape[0]
    ctx_rows = ext - 2 * HALO
    width, keys = value_p.shape[1], write_p.shape[1]
    blocks = tokens // BLOCK
    piece = 256
    modulate_into(latent, hidden, mod.at[0:1, :], mod.at[2:3, :])
    modulate_into(context_ext, hidden_c, mod.at[1:2, :], mod.at[3:4, :])

    def taps_at(ref, start):
        return ref[:, pl.ds(pl.multiple_of(start, piece), piece)]

    place = lax.broadcasted_iota(jnp.int32, (ext, piece), 0)
    live = ((place >= HALO) | (sp > 0)) & ((place < HALO + ctx_rows) | (sp < sp_n - 1))

    def latent_part(weight, taps, total, out):
        for c in range(0, total, piece):
            pre = jnp.dot(hidden[...], weight[:, c : c + piece], preferred_element_type=F32)
            pre = pre.astype(BF16)
            if taps is None:
                out[:, c : c + piece] = pre
            else:
                kernel = taps_at(taps, tp * total + c)
                out[:, c : c + piece] = conv_silu(pre.astype(F32), kernel, ROW)

    def context_part(weight, taps, total, out):
        for c in range(0, total, piece):
            pre = jnp.dot(hidden_c[...], weight[:, c : c + piece], preferred_element_type=F32)
            pre = jnp.where(live, pre.astype(BF16).astype(F32), 0.0)
            done = conv_silu(pre, taps_at(taps, tp * total + c), ext)
            out[:, c : c + piece] = done[HALO : HALO + ctx_rows]

    latent_part(value_p, value_t, width, values_o)
    latent_part(gate_p, None, width, gate_o)
    latent_part(write_p, write_t, keys, writes_o)
    latent_part(read_p, read_t, keys, reads_o)
    context_part(value_p, value_t, width, ctx_v)
    context_part(write_p, write_t, keys, ctx_w)
    raw = jnp.dot(hidden[...], step_p[...], preferred_element_type=F32).astype(BF16)
    pace = pacing[:, pl.ds(pl.multiple_of(sp * tokens, tokens), tokens)]
    pace = jnp.broadcast_to(pace, (LANES, tokens)).T
    step_o[...] = softplus(raw.astype(F32)) * pace
    raw_c = jnp.dot(hidden_c[...], step_p[...], preferred_element_type=F32).astype(BF16)
    step_c = softplus(raw_c.astype(F32))[HALO : HALO + ctx_rows]
    rate = rates[0:1, :]

    grand = jnp.zeros((1, LANES), F32)
    drops = []
    for k in range(blocks):
        at = slice(k * BLOCK, (k + 1) * BLOCK)
        step = step_o[at, :]
        decay = -rate * step
        cumul = running(decay, heads)
        total = jnp.sum(decay, axis=0, keepdims=True)
        cumul_o[at, :] = cumul
        weight = jnp.exp(total - cumul) * step
        grand += total
        drops.append(jnp.exp(total))
        found = partial_states(values_o[at, :], writes_o[at, :], weight, heads, per_group)
        for h in range(heads):
            inc_o[k, h * HEAD : (h + 1) * HEAD, :] = found[h]
    for h in range(heads):
        rows = slice(h * HEAD, (h + 1) * HEAD)
        forward = inc_o[0, rows, 0:STATE]
        for k in range(1, blocks):
            forward = drops[k][:, h : h + 1] * forward + inc_o[k, rows, 0:STATE]
        backward = inc_o[blocks - 1, rows, STATE : 2 * STATE]
        for k in range(blocks - 2, -1, -1):
            backward = (
                drops[k][:, heads + h : heads + h + 1] * backward
                + inc_o[k, rows, STATE : 2 * STATE])
        states_o[0, rows, :] = forward.astype(BF16)
        states_o[1, rows, :] = backward.astype(BF16)
    decay_c = -rate * step_c
    total_c = jnp.sum(decay_c, axis=0, keepdims=True)
    weight_c = jnp.exp(total_c - running(decay_c, heads)) * step_c
    found = partial_states(ctx_v[...], ctx_w[...], weight_c, heads, per_group)
    for h in range(heads):
        rows = slice(h * HEAD, (h + 1) * HEAD)
        states_o[2, rows, :] = found[h][:, 0:STATE].astype(BF16)
        states_o[3, rows, :] = found[h][:, STATE : 2 * STATE].astype(BF16)
    tots_o[0 : 2 * heads, :] = lane_to_rows(grand, 2 * heads)
    tots_o[2 * heads : 4 * heads, :] = lane_to_rows(total_c, 2 * heads)


def states_kernel(
    sp_n, heads,
    states, tots,
    starts,
    box, tot_box, outgoing,
    s1, r1, s2, r2, s3, r3,
):
    sp = lax.axis_index("sp")
    peers = others("sp", sp_n)
    share = states.shape[1] // sp_n
    greet([("sp", p) for p in peers])

    def rows_of(p):
        return pl.ds(pl.multiple_of(p * share, share), share)

    copies = []
    for d, p in enumerate(peers):
        copies.append(send(tots, tot_box.at[sp], s2.at[d], r2.at[d], "sp", p))
        copies.append(send(states.at[:, rows_of(p), :], box.at[sp], s1.at[d], r1.at[d], "sp", p))
    box[sp] = states[:, rows_of(sp), :]
    tot_box[sp] = tots[...]
    for copy in copies:
        copy.wait()
    first = (sp * share) // HEAD
    each = min(HEAD, share)

    def factor(j, base):
        rows = [
            jnp.broadcast_to(jnp.exp(tot_box[j, pl.ds(base + first + q, 1), :]), (each, STATE))
            for q in range(max(1, share // HEAD))
        ]
        return rows[0] if len(rows) == 1 else jnp.concatenate(rows, axis=0)

    forward = jnp.zeros((share, STATE), F32)
    for j in range(sp_n):
        forward = factor(j, 2 * heads) * forward + box[j, 2].astype(F32)
    backward = jnp.zeros((share, STATE), F32)
    for j in range(sp_n - 1, -1, -1):
        backward = factor(j, 3 * heads) * backward + box[j, 3].astype(F32)
    for j in range(sp_n):
        outgoing[j, 0] = forward.astype(BF16)
        forward = factor(j, 0) * forward + box[j, 0].astype(F32)
    for j in range(sp_n - 1, -1, -1):
        outgoing[j, 1] = backward.astype(BF16)
        backward = factor(j, heads) * backward + box[j, 1].astype(F32)
    back = [
        send(outgoing.at[p], starts.at[:, rows_of(sp), :], s3.at[d], r3.at[d], "sp", p)
        for d, p in enumerate(peers)
    ]
    starts[:, rows_of(sp), :] = outgoing[sp]
    for copy in back:
        copy.wait()


def sweep_kernel(
    heads, per_group,
    values, gate, writes, reads, step, cumul, inc, starts, gain, out_p,
    mixed_o,
    state_f, state_b, inner, joined,
):
    tp = lax.axis_index("tp")
    tokens = values.shape[0]
    width = values.shape[1]
    blocks = tokens // BLOCK
    span = per_group * HEAD
    groups = heads // per_group
    drops = [
        jnp.exp(jnp.where(
            lax.broadcasted_iota(jnp.int32, (1, LANES), 1) < heads,
            cumul[(k + 1) * BLOCK - 1 : (k + 1) * BLOCK, :],
            cumul[k * BLOCK : k * BLOCK + 1, :]))
        for k in range(blocks)
    ]
    for h in range(heads):
        rows = slice(h * HEAD, (h + 1) * HEAD)
        forward = starts[0, rows, :].astype(F32)
        for k in range(blocks):
            state_f[k, rows, :] = forward.astype(BF16)
            forward = drops[k][:, h : h + 1] * forward + inc[k, rows, 0:STATE]
        backward = starts[1, rows, :].astype(F32)
        for k in range(blocks - 1, -1, -1):
            state_b[k, rows, :] = backward.astype(BF16)
            backward = (
                drops[k][:, heads + h : heads + h + 1] * backward
                + inc[k, rows, STATE : 2 * STATE])
    at = lax.broadcasted_iota(jnp.int32, (BLOCK, BLOCK), 0)
    by = lax.broadcasted_iota(jnp.int32, (BLOCK, BLOCK), 1)
    past, diagonal = by <= at, by == at
    contract = (((1,), (1,)), ((), ()))

    def one_block(k, carry):
        rows = pl.ds(pl.multiple_of(k * BLOCK, BLOCK), BLOCK)
        c = cumul[rows, :]
        s = step[rows, :]
        c_turned, s_turned = c.T, s.T
        grown = jnp.exp(c)
        turned = values[rows, :].astype(F32).T.astype(BF16)
        for g in range(groups):
            read = reads[rows, g * STATE : (g + 1) * STATE]
            write = writes[rows, g * STATE : (g + 1) * STATE]
            affinity = lax.dot_general(read, write, contract, preferred_element_type=F32)
            read = read.astype(F32)
            for r in range(per_group):
                h = g * per_group + r
                b = heads + h
                head = slice(h * HEAD, (h + 1) * HEAD)
                exponent = jnp.where(
                    past,
                    c[:, h : h + 1] - c_turned[h : h + 1, :],
                    c[:, b : b + 1] - c_turned[b : b + 1, :])
                fs, bs = s_turned[h : h + 1, :], s_turned[b : b + 1, :]
                steps = jnp.where(past, fs, bs) + jnp.where(diagonal, bs, 0.0)
                mixing = (affinity * jnp.exp(exponent) * steps).astype(BF16)
                left = jnp.concatenate(
                    [mixing,
                     (read * grown[:, h : h + 1]).astype(BF16),
                     (read * grown[:, b : b + 1]).astype(BF16)], axis=1)
                right = jnp.concatenate(
                    [turned[head], state_f[k, head, :], state_b[k, head, :]], axis=1)
                joined[:, head] = lax.dot_general(
                    left, right, contract, preferred_element_type=F32)
            lanes = slice(g * span, (g + 1) * span)
            gated = joined[:, lanes] * silu(gate[rows, lanes].astype(F32))
            scale = lax.rsqrt(jnp.mean(gated * gated, -1, keepdims=True) + GATED_FLOOR)
            start = pl.multiple_of(tp * width + g * span, span)
            inner[rows, lanes] = (gated * scale * gain[:, pl.ds(start, span)]).astype(BF16)
        return carry

    lax.fori_loop(0, blocks, one_block, 0)
    piece = 512
    for c in range(0, out_p.shape[1], piece):
        mixed_o[:, c : c + piece] = jnp.dot(
            inner[...], out_p[:, c : c + piece], preferred_element_type=F32).astype(BF16)


def finish_kernel(tp_n, mixed, latent, mod, updated, box, ss, rs):
    tp = lax.axis_index("tp")
    peers = others("tp", tp_n)
    rows = latent.shape[0]
    greet([("tp", p) for p in peers])
    copies = [
        send(mixed.at[pl.ds(pl.multiple_of(p * rows, rows), rows)], box.at[d],
             ss.at[d], rs.at[d], "tp", p)
        for d, p in enumerate(peers)
    ]
    for copy in copies:
        copy.wait()
    tile_rows = 16

    def tile(i, carry):
        at = pl.ds(pl.multiple_of(i * tile_rows, tile_rows), tile_rows)
        own = pl.ds(pl.multiple_of(tp * rows + i * tile_rows, tile_rows), tile_rows)
        total = mixed[own, :].astype(F32)
        for d in range(tp_n - 1):
            total += box[d, at, :].astype(F32)
        total = total.astype(BF16).astype(F32)
        updated[at, :] = (latent[at, :].astype(F32) + mod[4:5, :] * total).astype(BF16)
        return carry

    lax.fori_loop(0, rows // tile_rows, tile, 0)


def shape(dims, kind):
    return jax.ShapeDtypeStruct(dims, kind)


def call(body, outs, count, scratch, collective=None, limit=60 << 20):
    params = dict(vmem_limit_bytes=limit)
    if collective is not None:
        params.update(collective_id=collective, has_side_effects=True)
    single = not isinstance(outs, (list, tuple))
    return pl.pallas_call(
        body,
        out_shape=outs,
        in_specs=[vmem()] * count,
        out_specs=vmem() if single else [vmem()] * len(outs),
        scratch_shapes=scratch,
        compiler_params=pltpu.CompilerParams(**params),
    )


def dma(count):
    return pltpu.SemaphoreType.DMA((count,))


def per_device(
    sp_n, tp_n,
    latent, condition, context, context_cond, shift_matrix, scale_matrix, gate_matrix,
    value_proj, gate_proj, write_proj, read_proj, step_proj, decay_rate, pacing,
    value_taps, write_taps, read_taps, norm_gain, out_proj,
):
    sp, tp = lax.axis_index("sp"), lax.axis_index("tp")
    rows, model = latent.shape[1:]
    ctx_rows = context.shape[1]
    tokens = rows * tp_n
    width, keys = value_proj.shape[1], write_proj.shape[1]
    heads = width // HEAD
    per_group = heads // (keys // STATE)
    blocks = tokens // BLOCK
    row_share = shift_matrix.shape[0]

    pair = jnp.stack([condition[0], context_cond])
    pair = lax.dynamic_slice_in_dim(pair, (sp * tp_n + tp) * row_share, row_share, 1)
    pair = jax.nn.silu(pair).astype(BF16)
    act = jnp.concatenate([
        jnp.pad(pair, ((0, 14), (0, 0))),
        jnp.pad(pair, ((2, 12), (0, 0))),
        jnp.pad(pair[:1], ((4, 11), (0, 0))),
    ])
    step_cols = lax.dynamic_slice_in_dim(step_proj, tp * heads, heads, 2)
    step_cols = jnp.pad(step_cols.reshape(model, 2 * heads), ((0, 0), (0, LANES - 2 * heads)))
    rates = lax.dynamic_slice_in_dim(decay_rate, tp * heads, heads, 1).reshape(1, 2 * heads)
    rates = jnp.pad(rates, ((0, 7), (0, LANES - 2 * heads)))

    latent_all, context_ext, mod = call(
        functools.partial(spread_kernel, sp_n, tp_n),
        [shape((tokens, model), BF16), shape((ctx_rows + 2 * HALO, model), BF16),
         shape((8, model), F32)],
        6,
        [pltpu.VMEM((8, model), F32), pltpu.VMEM((tp_n - 1, 8, model), F32),
         pltpu.VMEM((8, model), F32), pltpu.VMEM((sp_n - 1, 8, model), F32),
         dma(tp_n), dma(tp_n), dma(tp_n), dma(tp_n), dma(sp_n), dma(sp_n), dma(2), dma(2),
         dma(2)],
        0,
    )(act, shift_matrix, scale_matrix, gate_matrix, latent[0], context[0])

    values, gate, writes, reads, step, cumul, inc, states, tots = call(
        functools.partial(project_kernel, sp_n, heads, per_group),
        [shape((tokens, width), BF16), shape((tokens, width), BF16),
         shape((tokens, keys), BF16), shape((tokens, keys), BF16),
         shape((tokens, LANES), F32), shape((tokens, LANES), F32),
         shape((blocks, width, 2 * STATE), F32), shape((4, width, STATE), BF16),
         shape((4 * heads, LANES), F32)],
        13,
        [pltpu.VMEM((tokens, model), BF16), pltpu.VMEM((ctx_rows + 2 * HALO, model), BF16),
         pltpu.VMEM((ctx_rows, width), BF16), pltpu.VMEM((ctx_rows, keys), BF16)],
    )(latent_all, context_ext, mod, value_proj, gate_proj, write_proj, read_proj, step_cols,
      rates, pacing, value_taps, write_taps, read_taps)

    share = width // sp_n
    starts = call(
        functools.partial(states_kernel, sp_n, heads),
        shape((2, width, STATE), BF16),
        2,
        [pltpu.VMEM((sp_n, 4, share, STATE), BF16), pltpu.VMEM((sp_n, 4 * heads, LANES), F32),
         pltpu.VMEM((sp_n, 2, share, STATE), BF16),
         dma(sp_n), dma(sp_n), dma(sp_n), dma(sp_n), dma(sp_n), dma(sp_n)],
        1,
    )(states, tots)

    mixed = call(
        functools.partial(sweep_kernel, heads, per_group),
        shape((tokens, model), BF16),
        10,
        [pltpu.VMEM((blocks, width, STATE), BF16), pltpu.VMEM((blocks, width, STATE), BF16),
         pltpu.VMEM((tokens, width), BF16), pltpu.VMEM((BLOCK, width), F32)],
    )(values, gate, writes, reads, step, cumul, inc, starts, norm_gain[None], out_proj)

    updated = call(
        functools.partial(finish_kernel, tp_n),
        shape((rows, model), BF16),
        3,
        [pltpu.VMEM((tp_n - 1, rows, model), BF16), dma(tp_n), dma(tp_n)],
        2,
    )(mixed, latent[0], mod)
    return updated[None]


def solution(mesh):
    placed = (
        P("dp", ("sp", "tp"), None),
        P("dp", None),
        P("dp", "sp", None),
        P(),
        P(("sp", "tp"), None),
        P(("sp", "tp"), None),
        P(("sp", "tp"), None),
        P(None, "tp"),
        P(None, "tp"),
        P(None, "tp"),
        P(None, "tp"),
        P(),
        P(),
        P("dp", None),
        P(),
        P(),
        P(),
        P(),
        P("tp", None),
    )
    return jax.shard_map(
        functools.partial(per_device, mesh.shape["sp"], mesh.shape["tp"]),
        mesh=mesh,
        in_specs=placed,
        out_specs=P("dp", ("sp", "tp"), None),
        check_vma=False,
    )
```

```python
import functools

import jax
import jax.numpy as jnp
from jax import lax
from jax.experimental import pallas as pl
from jax.experimental.pallas import tpu as pltpu
from jax.sharding import PartitionSpec as P

HEAD = 64
STATE = 128
ROW = 64
BLOCK = 128
LANES = 128
HALO = 16

NORM_FLOOR = 1e-05
GATED_FLOOR = 1e-06
FINEST = lax.Precision.HIGHEST
MESH = pl.DeviceIdType.MESH
F32 = jnp.float32
BF16 = jnp.bfloat16


def vmem():
    return pl.BlockSpec(memory_space=pltpu.VMEM)


def send(src, dst, send_sem, recv_sem, axis, target):
    copy = pltpu.make_async_remote_copy(
        src_ref=src,
        dst_ref=dst,
        send_sem=send_sem,
        recv_sem=recv_sem,
        device_id={axis: target},
        device_id_type=MESH,
    )
    copy.start()
    return copy


def greet(peers):
    barrier = pltpu.get_barrier_semaphore()
    for axis, target in peers:
        pl.semaphore_signal(barrier, inc=1, device_id={axis: target}, device_id_type=MESH)
    pl.semaphore_wait(barrier, len(peers))


def others(axis, count):
    me = lax.axis_index(axis)
    return [lax.rem(me + d, count) for d in range(1, count)]


def ring_of(place, count):
    def turn(p):
        high, low = lax.div(p, 2), lax.rem(p, 2)
        return high * 2 + lax.rem(high + low, 2)

    spot = turn(place)
    return [turn(lax.rem(spot + d, count)) for d in (1, 3, 2)]


def softplus(x):
    return jnp.maximum(x, 0.0) + jnp.log1p(jnp.exp(-jnp.abs(x)))


def silu(x):
    return x * (1.0 / (1.0 + jnp.exp(-x)))


def modulate_into(source, target, shift_row, scale_row):
    step = 16

    def tile(i, carry):
        at = pl.ds(pl.multiple_of(i * step, step), step)
        values = source[at, :].astype(F32)
        center = jnp.mean(values, -1, keepdims=True)
        values = values - center
        spread = jnp.mean(values * values, -1, keepdims=True)
        normed = values * lax.rsqrt(spread + NORM_FLOOR)
        target[at, :] = (normed * (1.0 + scale_row[...]) + shift_row[...]).astype(BF16)
        return carry

    lax.fori_loop(0, source.shape[0] // step, tile, 0)


def conv_silu(values, taps, run):
    rows, channels = values.shape
    margin = taps.shape[0] // 2
    place = lax.broadcasted_iota(jnp.int32, (rows, channels), 0) % run
    summed = jnp.zeros((rows, channels), F32)
    for k in range(taps.shape[0]):
        offset = k - margin
        moved = pltpu.roll(values, (-offset) % rows, 0) if offset else values
        if offset:
            moved = jnp.where((place + offset >= 0) & (place + offset < run), moved, 0.0)
        summed += moved * taps[k : k + 1, :]
    return silu(summed).astype(BF16)


def running(decay, heads):
    rows = decay.shape[0]
    at = lax.broadcasted_iota(jnp.int32, (rows, rows), 0)
    by = lax.broadcasted_iota(jnp.int32, (rows, rows), 1)
    lower = (by <= at).astype(F32)
    upper = (by >= at).astype(F32)
    lane = lax.broadcasted_iota(jnp.int32, decay.shape, 1)
    forward = jnp.dot(lower, decay, precision=FINEST, preferred_element_type=F32)
    backward = jnp.dot(upper, decay, precision=FINEST, preferred_element_type=F32)
    return jnp.where(lane < heads, forward, backward)


def lane_to_rows(row, count):
    return jnp.broadcast_to(row, (LANES, LANES)).T[0:count]


def partial_states(values, writes, weight, heads, per_group):
    turned = values.astype(F32).T.astype(BF16)
    result = []
    for h in range(heads):
        g = h // per_group
        rows = writes[:, g * STATE : (g + 1) * STATE].astype(F32)
        pair = jnp.concatenate(
            [(rows * weight[:, h : h + 1]).astype(BF16),
             (rows * weight[:, heads + h : heads + h + 1]).astype(BF16)], axis=1)
        result.append(
            jnp.dot(turned[h * HEAD : (h + 1) * HEAD], pair, preferred_element_type=F32))
    return result


def front_kernel(
    sp_n, tp_n, heads, per_group,
    act, shift_m, scale_m, gate_m, latent, context,
    value_h, gate_h, write_h, read_h, step_p, rates, pacing, value_t, write_t, read_t,
    values_o, gate_o, writes_o, reads_o, step_o, cumul_o, inc_o, ends_o, ctx_o, mod,
    value_p, gate_p, write_p, read_p,
    latent_all, context_ext, part, tp_box, middle, sp_box,
    hidden, hidden_c, ctx_v, ctx_w,
    c_states, c_tots, c_box, c_tot_box, c_out,
    own, lat_s, lat_r, tps, tpr, sps, spr, halo_s, halo_r, s1, r1, s2, r2, s3, r3,
):
    sp, tp = lax.axis_index("sp"), lax.axis_index("tp")
    tp_peers, sp_peers = others("tp", tp_n), others("sp", sp_n)
    rows, ctx_rows = latent.shape[0], context.shape[0]
    tokens, model = latent_all.shape
    ext = context_ext.shape[0]
    width, keys = value_p.shape[1], write_p.shape[1]
    blocks = tokens // BLOCK
    piece = 256
    loads = [
        pltpu.make_async_copy(src, dst, own.at[2 + i])
        for i, (src, dst) in enumerate(
            [(value_h, value_p), (write_h, write_p), (gate_h, gate_p), (read_h, read_p)])
    ]
    for copy in loads:
        copy.start()
    greet([("tp", p) for p in tp_peers] + [("sp", p) for p in sp_peers])

    def rows_at(p, count, start=0):
        return pl.ds(pl.multiple_of(p * rows + start, count), count)

    mine = rows_at(tp, rows)
    copy_lat = pltpu.make_async_copy(latent, latent_all.at[mine], own.at[0])
    copy_lat.start()
    copy_ctx = pltpu.make_async_copy(context, context_ext.at[pl.ds(HALO, ctx_rows)], own.at[1])
    copy_ctx.start()
    before = lax.rem(sp + sp_n - 1, sp_n)
    after = lax.rem(sp + 1, sp_n)
    halos = [
        send(context.at[pl.ds(ctx_rows - HALO, HALO)], context_ext.at[pl.ds(0, HALO)],
             halo_s.at[0], halo_r.at[0], "sp", after),
        send(context.at[pl.ds(0, HALO)], context_ext.at[pl.ds(HALO + ctx_rows, HALO)],
             halo_s.at[1], halo_r.at[1], "sp", before),
    ]
    total = jnp.dot(act[0:16, :], shift_m[...], preferred_element_type=F32)
    total += jnp.dot(act[16:32, :], scale_m[...], preferred_element_type=F32)
    total += jnp.dot(act[32:48, :], gate_m[...], preferred_element_type=F32)
    for c in range(model // LANES):
        part[5 * c : 5 * c + 5, :] = total[0:5, c * LANES : (c + 1) * LANES]
    first = [
        send(part, tp_box.at[d], tps.at[d], tpr.at[d], "tp", p) for d, p in enumerate(tp_peers)
    ]
    if tp_n == 4:
        right, left, opposite = ring_of(tp, tp_n)
        to_right = send(latent, latent_all.at[mine], lat_s.at[0], lat_r.at[0], "tp", right)
        to_left = send(latent, latent_all.at[mine], lat_s.at[1], lat_r.at[1], "tp", left)
        moves = [to_right, to_left]
    else:
        moves = [
            send(latent, latent_all.at[mine], lat_s.at[d], lat_r.at[d], "tp", p)
            for d, p in enumerate(tp_peers)
        ]
    for copy in first:
        copy.wait()
    summed = part[...]
    for d in range(tp_n - 1):
        summed += tp_box[d]
    middle[...] = summed
    second = [
        send(middle, sp_box.at[d], sps.at[d], spr.at[d], "sp", p) for d, p in enumerate(sp_peers)
    ]
    for copy in second:
        copy.wait()
    summed = middle[...]
    for d in range(sp_n - 1):
        summed += sp_box[d]
    middle[...] = summed
    mod[...] = jnp.zeros_like(mod)
    for c in range(model // LANES):
        mod[0:5, c * LANES : (c + 1) * LANES] = middle[5 * c : 5 * c + 5, :]
    for copy in halos:
        copy.wait()
    copy_lat.wait()
    copy_ctx.wait()
    if tp_n == 4:
        half = rows // 2
        to_right.wait()
        on_right = send(latent_all.at[rows_at(left, half)], latent_all.at[rows_at(left, half)],
                        lat_s.at[2], lat_r.at[2], "tp", right)
        to_left.wait()
        on_left = send(latent_all.at[rows_at(right, half, half)],
                       latent_all.at[rows_at(right, half, half)],
                       lat_s.at[3], lat_r.at[3], "tp", left)
        moves = [on_right, on_left]

    modulate_into(context_ext, hidden_c, mod.at[1:2, :], mod.at[3:4, :])

    def taps_at(ref, start):
        return ref[:, pl.ds(pl.multiple_of(start, piece), piece)]

    place = lax.broadcasted_iota(jnp.int32, (ext, piece), 0)
    live = ((place >= HALO) | (sp > 0)) & ((place < HALO + ctx_rows) | (sp < sp_n - 1))

    def latent_part(weight, taps, total, out):
        for c in range(0, total, piece):
            pre = jnp.dot(hidden[...], weight[:, c : c + piece], preferred_element_type=F32)
            pre = pre.astype(BF16)
            if taps is None:
                out[:, c : c + piece] = pre
            else:
                kernel = taps_at(taps, tp * total + c)
                out[:, c : c + piece] = conv_silu(pre.astype(F32), kernel, ROW)

    def context_part(weight, taps, total, out):
        for c in range(0, total, piece):
            pre = jnp.dot(hidden_c[...], weight[:, c : c + piece], preferred_element_type=F32)
            pre = jnp.where(live, pre.astype(BF16).astype(F32), 0.0)
            done = conv_silu(pre, taps_at(taps, tp * total + c), ext)
            out[:, c : c + piece] = done[HALO : HALO + ctx_rows]

    rate = rates[0:1, :]
    loads[0].wait()
    loads[1].wait()
    context_part(value_p, value_t, width, ctx_v)
    context_part(write_p, write_t, keys, ctx_w)
    raw_c = jnp.dot(hidden_c[...], step_p[...], preferred_element_type=F32).astype(BF16)
    step_c = softplus(raw_c.astype(F32))[HALO : HALO + ctx_rows]
    decay_c = -rate * step_c
    total_c = jnp.sum(decay_c, axis=0, keepdims=True)
    weight_c = jnp.exp(total_c - running(decay_c, heads)) * step_c
    found = partial_states(ctx_v[...], ctx_w[...], weight_c, heads, per_group)
    for h in range(heads):
        at = slice(h * HEAD, (h + 1) * HEAD)
        c_states[0, at, :] = found[h][:, 0:STATE].astype(BF16)
        c_states[1, at, :] = found[h][:, STATE : 2 * STATE].astype(BF16)
    c_tots[...] = lane_to_rows(total_c, 2 * heads)

    share = width // sp_n

    def share_of(p):
        return pl.ds(pl.multiple_of(p * share, share), share)

    gathers = []
    for d, p in enumerate(sp_peers):
        gathers.append(send(c_tots, c_tot_box.at[sp], s2.at[d], r2.at[d], "sp", p))
        gathers.append(
            send(c_states.at[:, share_of(p), :], c_box.at[sp], s1.at[d], r1.at[d], "sp", p))
    c_box[sp] = c_states[:, share_of(sp), :]
    c_tot_box[sp] = c_tots[...]

    for copy in moves:
        copy.wait()
    modulate_into(latent_all, hidden, mod.at[0:1, :], mod.at[2:3, :])

    for copy in gathers:
        copy.wait()
    head_at = (sp * share) // HEAD
    each = min(HEAD, share)

    def factor(j, base):
        found = [
            jnp.broadcast_to(
                jnp.exp(c_tot_box[j, pl.ds(base + head_at + q, 1), :]), (each, STATE))
            for q in range(max(1, share // HEAD))
        ]
        return found[0] if len(found) == 1 else jnp.concatenate(found, axis=0)

    forward = jnp.zeros((share, STATE), F32)
    for j in range(sp_n):
        forward = factor(j, 0) * forward + c_box[j, 0].astype(F32)
    backward = jnp.zeros((share, STATE), F32)
    for j in range(sp_n - 1, -1, -1):
        backward = factor(j, heads) * backward + c_box[j, 1].astype(F32)
    c_out[0] = forward.astype(BF16)
    c_out[1] = backward.astype(BF16)
    back = [
        send(c_out, ctx_o.at[:, share_of(sp), :], s3.at[d], r3.at[d], "sp", p)
        for d, p in enumerate(sp_peers)
    ]
    ctx_o[:, share_of(sp), :] = c_out[...]

    latent_part(value_p, value_t, width, values_o)
    latent_part(write_p, write_t, keys, writes_o)
    loads[2].wait()
    loads[3].wait()
    latent_part(gate_p, None, width, gate_o)
    latent_part(read_p, read_t, keys, reads_o)
    raw = jnp.dot(hidden[...], step_p[...], preferred_element_type=F32).astype(BF16)
    pace = pacing[:, pl.ds(pl.multiple_of(sp * tokens, tokens), tokens)]
    pace = jnp.broadcast_to(pace, (LANES, tokens)).T
    step_o[...] = softplus(raw.astype(F32)) * pace
    drops = []
    for k in range(blocks):
        at = slice(k * BLOCK, (k + 1) * BLOCK)
        step = step_o[at, :]
        decay = -rate * step
        cumul = running(decay, heads)
        total = jnp.sum(decay, axis=0, keepdims=True)
        cumul_o[at, :] = cumul
        weight = jnp.exp(total - cumul) * step
        drops.append(jnp.exp(total))
        found = partial_states(values_o[at, :], writes_o[at, :], weight, heads, per_group)
        for h in range(heads):
            inc_o[k, h * HEAD : (h + 1) * HEAD, :] = found[h]
    for h in range(heads):
        at = slice(h * HEAD, (h + 1) * HEAD)
        forward = inc_o[0, at, 0:STATE]
        for k in range(1, blocks):
            forward = drops[k][:, h : h + 1] * forward + inc_o[k, at, 0:STATE]
        backward = inc_o[blocks - 1, at, STATE : 2 * STATE]
        for k in range(blocks - 2, -1, -1):
            backward = (
                drops[k][:, heads + h : heads + h + 1] * backward
                + inc_o[k, at, STATE : 2 * STATE])
        ends_o[0, at, :] = forward
        ends_o[1, at, :] = backward
    for copy in back:
        copy.wait()


def sweep_kernel(
    sp_n, heads, per_group,
    values, gate, writes, reads, step, cumul, inc, ends, ctx, gain,
    inner,
    starts, outgoing, state_f, state_b, joined, ss, rs,
):
    sp, tp = lax.axis_index("sp"), lax.axis_index("tp")
    tokens, width = values.shape
    blocks = tokens // BLOCK
    span = per_group * HEAD
    groups = heads // per_group
    after, before = lax.rem(sp + 1, sp_n), lax.rem(sp + sp_n - 1, sp_n)
    greet([("sp", after), ("sp", before)])
    lane = lax.broadcasted_iota(jnp.int32, (1, LANES), 1)
    totals = [
        jnp.where(
            lane < heads,
            cumul[(k + 1) * BLOCK - 1 : (k + 1) * BLOCK, :],
            cumul[k * BLOCK : k * BLOCK + 1, :])
        for k in range(blocks)
    ]
    drops = [jnp.exp(t) for t in totals]
    grand = totals[0]
    for t in totals[1:]:
        grand = grand + t
    grand = jnp.exp(grand)
    chunk = 2 * HEAD
    chunks = width // chunk

    def link(way, c):
        at = pl.ds(c * chunk, chunk)
        return pltpu.make_async_remote_copy(
            src_ref=outgoing.at[way, at],
            dst_ref=starts.at[way, at],
            send_sem=ss.at[way * chunks + c],
            recv_sem=rs.at[way * chunks + c],
            device_id={"sp": before if way else after},
            device_id_type=MESH,
        )

    def chain(way):
        enters = sp == (sp_n - 1 if way else 0)
        leaves = sp == (0 if way else sp_n - 1)

        @pl.when(enters)
        def _():
            starts[way] = ctx[way]

        for c in range(chunks):
            @pl.when(jnp.logical_not(enters))
            def _():
                link(way, c).wait_recv()

            @pl.when(jnp.logical_not(leaves))
            def _():
                for q in range(chunk // HEAD):
                    h = c * (chunk // HEAD) + q
                    at = slice(h * HEAD, (h + 1) * HEAD)
                    j = way * heads + h
                    outgoing[way, at, :] = (
                        grand[:, j : j + 1] * starts[way, at, :].astype(F32) + ends[way, at, :]
                    ).astype(BF16)
                link(way, c).start()

    at_row = lax.broadcasted_iota(jnp.int32, (BLOCK, BLOCK), 0)
    by_row = lax.broadcasted_iota(jnp.int32, (BLOCK, BLOCK), 1)
    past, diagonal = by_row <= at_row, by_row == at_row
    contract = (((1,), (1,)), ((), ()))

    def local_block(k):
        rows = slice(k * BLOCK, (k + 1) * BLOCK)
        c = cumul[rows, :]
        c_turned, s_turned = c.T, step[rows, :].T
        for g in range(groups):
            keys = slice(g * STATE, (g + 1) * STATE)
            affinity = lax.dot_general(
                reads[rows, keys], writes[rows, keys], contract, preferred_element_type=F32)
            for r in range(per_group):
                h = g * per_group + r
                b = heads + h
                head = slice(h * HEAD, (h + 1) * HEAD)
                exponent = jnp.where(
                    past,
                    c[:, h : h + 1] - c_turned[h : h + 1, :],
                    c[:, b : b + 1] - c_turned[b : b + 1, :])
                fs, bs = s_turned[h : h + 1, :], s_turned[b : b + 1, :]
                steps = jnp.where(past, fs, bs) + jnp.where(diagonal, bs, 0.0)
                mixing = (affinity * jnp.exp(exponent) * steps).astype(BF16)
                joined[rows, head] = jnp.dot(
                    mixing, values[rows, head], preferred_element_type=F32)

    for slot in range(blocks):
        last = slot == blocks - 1
        for way in range(2):
            turn = (sp_n - 1 - sp) if way else sp
            pl.when(turn >= slot if last else turn == slot)(functools.partial(chain, way))
        local_block(slot)

    for way in range(2):
        @pl.when(sp != (0 if way else sp_n - 1))
        def _():
            for c in range(chunks):
                link(way, c).wait_send()

    for h in range(heads):
        rows = slice(h * HEAD, (h + 1) * HEAD)
        forward = starts[0, rows, :].astype(F32)
        for k in range(blocks):
            state_f[k, rows, :] = forward.astype(BF16)
            forward = drops[k][:, h : h + 1] * forward + inc[k, rows, 0:STATE]
        backward = starts[1, rows, :].astype(F32)
        for k in range(blocks - 1, -1, -1):
            state_b[k, rows, :] = backward.astype(BF16)
            backward = (
                drops[k][:, heads + h : heads + h + 1] * backward
                + inc[k, rows, STATE : 2 * STATE])

    def carried_block(k, carry):
        rows = pl.ds(pl.multiple_of(k * BLOCK, BLOCK), BLOCK)
        grown = jnp.exp(cumul[rows, :])
        for g in range(groups):
            read = reads[rows, g * STATE : (g + 1) * STATE].astype(F32)
            for r in range(per_group):
                h = g * per_group + r
                b = heads + h
                head = slice(h * HEAD, (h + 1) * HEAD)
                left = jnp.concatenate(
                    [(read * grown[:, h : h + 1]).astype(BF16),
                     (read * grown[:, b : b + 1]).astype(BF16)], axis=1)
                right = jnp.concatenate([state_f[k, head, :], state_b[k, head, :]], axis=1)
                joined[rows, head] += lax.dot_general(
                    left, right, contract, preferred_element_type=F32)
            lanes = slice(g * span, (g + 1) * span)
            gated = joined[rows, lanes] * silu(gate[rows, lanes].astype(F32))
            scale = lax.rsqrt(jnp.mean(gated * gated, -1, keepdims=True) + GATED_FLOOR)
            start = pl.multiple_of(tp * width + g * span, span)
            inner[rows, lanes] = (gated * scale * gain[:, pl.ds(start, span)]).astype(BF16)
        return carry

    lax.fori_loop(0, blocks, carried_block, 0)


def finish_kernel(tp_n, inner, out_p, total_o, mixed, early, relay, box, ss, rs):
    tp = lax.axis_index("tp")
    peers = others("tp", tp_n)
    rows, model = total_o.shape
    greet([("tp", p) for p in peers])

    def product(owner):
        at = pl.ds(pl.multiple_of(owner * rows, rows), rows)
        for c in range(0, model, 512):
            mixed[at, c : c + 512] = jnp.dot(
                inner[at, :], out_p[:, c : c + 512], preferred_element_type=F32).astype(BF16)

    def rows_at(p, count, start=0):
        return pl.ds(pl.multiple_of(p * rows + start, count), count)

    if tp_n == 4:
        half = rows // 2
        low, high = pl.ds(0, half), pl.ds(half, half)
        right, left, opposite = ring_of(tp, tp_n)
        product(opposite)
        far = [
            send(mixed.at[rows_at(opposite, half)], early.at[0], ss.at[0], rs.at[0], "tp", right),
            send(mixed.at[rows_at(opposite, half, half)], early.at[1],
                 ss.at[1], rs.at[1], "tp", left),
        ]
        product(right)
        copies = [send(mixed.at[rows_at(right, half, half)], box.at[0, high],
                       ss.at[2], rs.at[2], "tp", right)]
        product(left)
        copies.append(send(mixed.at[rows_at(left, half)], box.at[1, low],
                           ss.at[3], rs.at[3], "tp", left))
        product(tp)
        for way, (owner, start, lands) in enumerate([(right, 0, low), (left, half, high)]):
            far[way].wait()
            relay[way] = (
                mixed[rows_at(owner, half, start), :].astype(F32) + early[way].astype(F32)
            ).astype(BF16)
            copies.append(send(relay.at[way], box.at[way, lands],
                               ss.at[4 + way], rs.at[4 + way], "tp", owner))
        landed = 2
    else:
        for p in peers + [tp]:
            product(p)
        copies = [
            send(mixed.at[rows_at(p, rows)], box.at[d], ss.at[d], rs.at[d], "tp", p)
            for d, p in enumerate(peers)
        ]
        landed = tp_n - 1
    for copy in copies:
        copy.wait()
    tile_rows = 16

    def tile(i, carry):
        at = pl.ds(pl.multiple_of(i * tile_rows, tile_rows), tile_rows)
        own = pl.ds(pl.multiple_of(tp * rows + i * tile_rows, tile_rows), tile_rows)
        total = mixed[own, :].astype(F32)
        for d in range(landed):
            total += box[d, at, :].astype(F32)
        total_o[at, :] = total.astype(BF16)
        return carry

    lax.fori_loop(0, rows // tile_rows, tile, 0)


def shape(dims, kind):
    return jax.ShapeDtypeStruct(dims, kind)


def call(body, outs, specs, scratch, collective, limit=60 << 20):
    params = dict(vmem_limit_bytes=limit, collective_id=collective, has_side_effects=True)
    single = not isinstance(outs, (list, tuple))
    return pl.pallas_call(
        body,
        out_shape=outs,
        in_specs=specs,
        out_specs=vmem() if single else [vmem()] * len(outs),
        scratch_shapes=scratch,
        compiler_params=pltpu.CompilerParams(**params),
    )


def dma(count):
    return pltpu.SemaphoreType.DMA((count,))


def per_device(
    sp_n, tp_n,
    latent, condition, context, context_cond, shift_matrix, scale_matrix, gate_matrix,
    value_proj, gate_proj, write_proj, read_proj, step_proj, decay_rate, pacing,
    value_taps, write_taps, read_taps, norm_gain, out_proj,
):
    sp, tp = lax.axis_index("sp"), lax.axis_index("tp")
    rows, model = latent.shape[1:]
    ctx_rows = context.shape[1]
    tokens = rows * tp_n
    width, keys = value_proj.shape[1], write_proj.shape[1]
    heads = width // HEAD
    per_group = heads // (keys // STATE)
    blocks = tokens // BLOCK
    row_share = shift_matrix.shape[0]

    pair = jnp.stack([condition[0], context_cond])
    pair = lax.dynamic_slice_in_dim(pair, (sp * tp_n + tp) * row_share, row_share, 1)
    pair = jax.nn.silu(pair).astype(BF16)
    act = jnp.concatenate([
        jnp.pad(pair, ((0, 14), (0, 0))),
        jnp.pad(pair, ((2, 12), (0, 0))),
        jnp.pad(pair[:1], ((4, 11), (0, 0))),
    ])
    step_cols = lax.dynamic_slice_in_dim(step_proj, tp * heads, heads, 2)
    step_cols = jnp.pad(step_cols.reshape(model, 2 * heads), ((0, 0), (0, LANES - 2 * heads)))
    rates = lax.dynamic_slice_in_dim(decay_rate, tp * heads, heads, 1).reshape(1, 2 * heads)
    rates = jnp.pad(rates, ((0, 7), (0, LANES - 2 * heads)))

    held = pl.BlockSpec(memory_space=pl.ANY)
    ext = ctx_rows + 2 * HALO
    share = width // sp_n
    packed = 5 * model // LANES
    values, gate, writes, reads, step, cumul, inc, ends, ctx, mod = call(
        functools.partial(front_kernel, sp_n, tp_n, heads, per_group),
        [shape((tokens, width), BF16), shape((tokens, width), BF16),
         shape((tokens, keys), BF16), shape((tokens, keys), BF16),
         shape((tokens, LANES), F32), shape((tokens, LANES), F32),
         shape((blocks, width, 2 * STATE), F32), shape((2, width, STATE), F32),
         shape((2, width, STATE), BF16), shape((8, model), F32)],
        [vmem()] * 6 + [held] * 4 + [vmem()] * 6,
        [pltpu.VMEM((model, width), BF16), pltpu.VMEM((model, width), BF16),
         pltpu.VMEM((model, keys), BF16), pltpu.VMEM((model, keys), BF16),
         pltpu.VMEM((tokens, model), BF16), pltpu.VMEM((ext, model), BF16),
         pltpu.VMEM((packed, LANES), F32), pltpu.VMEM((tp_n - 1, packed, LANES), F32),
         pltpu.VMEM((packed, LANES), F32), pltpu.VMEM((sp_n - 1, packed, LANES), F32),
         pltpu.VMEM((tokens, model), BF16), pltpu.VMEM((ext, model), BF16),
         pltpu.VMEM((ctx_rows, width), BF16), pltpu.VMEM((ctx_rows, keys), BF16),
         pltpu.VMEM((2, width, STATE), BF16), pltpu.VMEM((2 * heads, LANES), F32),
         pltpu.VMEM((sp_n, 2, share, STATE), BF16), pltpu.VMEM((sp_n, 2 * heads, LANES), F32),
         pltpu.VMEM((2, share, STATE), BF16),
         dma(6), dma(tp_n), dma(tp_n), dma(tp_n), dma(tp_n), dma(sp_n), dma(sp_n), dma(2), dma(2),
         dma(sp_n), dma(sp_n), dma(sp_n), dma(sp_n), dma(sp_n), dma(sp_n)],
        0,
    )(act, shift_matrix, scale_matrix, gate_matrix, latent[0], context[0],
      value_proj, gate_proj, write_proj, read_proj, step_cols,
      rates, pacing, value_taps, write_taps, read_taps)

    pieces = 2 * (width // (2 * HEAD))
    inner = call(
        functools.partial(sweep_kernel, sp_n, heads, per_group),
        shape((tokens, width), BF16),
        [vmem()] * 10,
        [pltpu.VMEM((2, width, STATE), BF16), pltpu.VMEM((2, width, STATE), BF16),
         pltpu.VMEM((blocks, width, STATE), BF16), pltpu.VMEM((blocks, width, STATE), BF16),
         pltpu.VMEM((tokens, width), F32), dma(pieces), dma(pieces)],
        1,
    )(values, gate, writes, reads, step, cumul, inc, ends, ctx, norm_gain[None])

    total = call(
        functools.partial(finish_kernel, tp_n),
        shape((rows, model), BF16),
        [vmem()] * 2,
        [pltpu.VMEM((tokens, model), BF16), pltpu.VMEM((2, rows // 2, model), BF16),
         pltpu.VMEM((2, rows // 2, model), BF16), pltpu.VMEM((tp_n - 1, rows, model), BF16),
         dma(6), dma(6)],
        2,
    )(inner, out_proj)
    updated = latent[0].astype(F32) + mod[4:5] * lax.optimization_barrier(total).astype(F32)
    return updated.astype(BF16)[None]


def solution(mesh):
    placed = (
        P("dp", ("sp", "tp"), None),
        P("dp", None),
        P("dp", "sp", None),
        P(),
        P(("sp", "tp"), None),
        P(("sp", "tp"), None),
        P(("sp", "tp"), None),
        P(None, "tp"),
        P(None, "tp"),
        P(None, "tp"),
        P(None, "tp"),
        P(),
        P(),
        P("dp", None),
        P(),
        P(),
        P(),
        P(),
        P("tp", None),
    )
    return jax.shard_map(
        functools.partial(per_device, mesh.shape["sp"], mesh.shape["tp"]),
        mesh=mesh,
        in_specs=placed,
        out_specs=P("dp", ("sp", "tp"), None),
        check_vma=False,
    )
```

```python
import functools

import jax
import jax.numpy as jnp
from jax import lax
from jax.experimental import pallas as pl
from jax.experimental.pallas import tpu as pltpu
from jax.sharding import PartitionSpec as P

HEAD = 64
STATE = 128
ROW = 64
BLOCK = 128
LANES = 128
HALO = 16
FRONT = 34

NORM_FLOOR = 1e-05
GATED_FLOOR = 1e-06
FINEST = lax.Precision.HIGHEST
MESH = pl.DeviceIdType.MESH
F32 = jnp.float32
BF16 = jnp.bfloat16


def vmem():
    return pl.BlockSpec(memory_space=pltpu.VMEM)


def send(src, dst, send_sem, recv_sem, axis, target):
    copy = pltpu.make_async_remote_copy(
        src_ref=src,
        dst_ref=dst,
        send_sem=send_sem,
        recv_sem=recv_sem,
        device_id={axis: target},
        device_id_type=MESH,
    )
    copy.start()
    return copy


def greet(peers):
    barrier = pltpu.get_barrier_semaphore()
    for axis, target in peers:
        pl.semaphore_signal(barrier, inc=1, device_id={axis: target}, device_id_type=MESH)
    pl.semaphore_wait(barrier, len(peers))


def others(axis, count):
    me = lax.axis_index(axis)
    return [lax.rem(me + d, count) for d in range(1, count)]


def ring_of(place, count):
    def turn(p):
        high, low = lax.div(p, 2), lax.rem(p, 2)
        return high * 2 + lax.rem(high + low, 2)

    spot = turn(place)
    return [turn(lax.rem(spot + d, count)) for d in (1, 3, 2)]


def softplus(x):
    return jnp.maximum(x, 0.0) + jnp.log1p(jnp.exp(-jnp.abs(x)))


def silu(x):
    return x * (1.0 / (1.0 + jnp.exp(-x)))


def modulate_into(source, target, shift_row, scale_row):
    step = 16

    def tile(i, carry):
        at = pl.ds(pl.multiple_of(i * step, step), step)
        values = source[at, :].astype(F32)
        center = jnp.mean(values, -1, keepdims=True)
        values = values - center
        spread = jnp.mean(values * values, -1, keepdims=True)
        normed = values * lax.rsqrt(spread + NORM_FLOOR)
        target[at, :] = (normed * (1.0 + scale_row[...]) + shift_row[...]).astype(BF16)
        return carry

    lax.fori_loop(0, source.shape[0] // step, tile, 0)


def conv_silu(values, taps, run):
    rows, channels = values.shape
    margin = taps.shape[0] // 2
    place = lax.broadcasted_iota(jnp.int32, (rows, channels), 0) % run
    summed = jnp.zeros((rows, channels), F32)
    for k in range(taps.shape[0]):
        offset = k - margin
        moved = pltpu.roll(values, (-offset) % rows, 0) if offset else values
        if offset:
            moved = jnp.where((place + offset >= 0) & (place + offset < run), moved, 0.0)
        summed += moved * taps[k : k + 1, :]
    return silu(summed).astype(BF16)


def running(decay, heads):
    rows = decay.shape[0]
    at = lax.broadcasted_iota(jnp.int32, (rows, rows), 0)
    by = lax.broadcasted_iota(jnp.int32, (rows, rows), 1)
    lower = (by <= at).astype(F32)
    upper = (by >= at).astype(F32)
    lane = lax.broadcasted_iota(jnp.int32, decay.shape, 1)
    forward = jnp.dot(lower, decay, precision=FINEST, preferred_element_type=F32)
    backward = jnp.dot(upper, decay, precision=FINEST, preferred_element_type=F32)
    return jnp.where(lane < heads, forward, backward)


def lane_to_rows(row, count):
    return jnp.broadcast_to(row, (LANES, LANES)).T[0:count]


def partial_states(values, writes, weight, heads, per_group):
    turned = values.astype(F32).T.astype(BF16)
    result = []
    for h in range(heads):
        g = h // per_group
        rows = writes[:, g * STATE : (g + 1) * STATE].astype(F32)
        pair = jnp.concatenate(
            [(rows * weight[:, h : h + 1]).astype(BF16),
             (rows * weight[:, heads + h : heads + h + 1]).astype(BF16)], axis=1)
        result.append(
            jnp.dot(turned[h * HEAD : (h + 1) * HEAD], pair, preferred_element_type=F32))
    return result


def front_kernel(
    sp_n, tp_n, heads, per_group,
    act, shift_m, scale_m, gate_m, latent, context,
    value_h, gate_h, write_h, read_h, step_p, rates, pacing, value_t, write_t, read_t,
    values_o, gate_o, writes_o, reads_o, step_o, cumul_o, inc_o, ends_o, ctx_o, mod,
    value_p, gate_p, write_p, read_p,
    latent_all, context_ext, part, tp_box, middle, sp_box,
    hidden, hidden_c, ctx_v, ctx_w,
    c_states, c_tots, c_box, c_tot_box, c_out,
    own, lat_s, lat_r, tps, tpr, sps, spr, halo_s, halo_r, s1, r1, s2, r2, s3, r3,
):
    sp, tp = lax.axis_index("sp"), lax.axis_index("tp")
    tp_peers, sp_peers = others("tp", tp_n), others("sp", sp_n)
    rows, ctx_rows = latent.shape[0], context.shape[0]
    tokens, model = latent_all.shape
    ext = context_ext.shape[0]
    width, keys = value_p.shape[1], write_p.shape[1]
    blocks = tokens // BLOCK
    piece = 256
    loads = [
        pltpu.make_async_copy(src, dst, own.at[2 + i])
        for i, (src, dst) in enumerate(
            [(value_h, value_p), (write_h, write_p), (gate_h, gate_p), (read_h, read_p)])
    ]
    for copy in loads:
        copy.start()
    greet([("tp", p) for p in tp_peers] + [("sp", p) for p in sp_peers])

    def rows_at(p, count, start=0):
        return pl.ds(pl.multiple_of(p * rows + start, count), count)

    mine = rows_at(tp, rows)
    copy_lat = pltpu.make_async_copy(latent, latent_all.at[mine], own.at[0])
    copy_lat.start()
    copy_ctx = pltpu.make_async_copy(context, context_ext.at[pl.ds(HALO, ctx_rows)], own.at[1])
    copy_ctx.start()
    before = lax.rem(sp + sp_n - 1, sp_n)
    after = lax.rem(sp + 1, sp_n)
    halos = [
        send(context.at[pl.ds(ctx_rows - HALO, HALO)], context_ext.at[pl.ds(0, HALO)],
             halo_s.at[0], halo_r.at[0], "sp", after),
        send(context.at[pl.ds(0, HALO)], context_ext.at[pl.ds(HALO + ctx_rows, HALO)],
             halo_s.at[1], halo_r.at[1], "sp", before),
    ]
    total = jnp.dot(act[0:16, :], shift_m[...], preferred_element_type=F32)
    total += jnp.dot(act[16:32, :], scale_m[...], preferred_element_type=F32)
    total += jnp.dot(act[32:48, :], gate_m[...], preferred_element_type=F32)
    for c in range(model // LANES):
        part[5 * c : 5 * c + 5, :] = total[0:5, c * LANES : (c + 1) * LANES]
    first = [
        send(part, tp_box.at[d], tps.at[d], tpr.at[d], "tp", p) for d, p in enumerate(tp_peers)
    ]
    if tp_n == 4:
        right, left, opposite = ring_of(tp, tp_n)
        half = rows // 2

        def pass_on(owner, start, target, i):
            at = rows_at(owner, half, start)
            src = latent.at[pl.ds(start, half)] if owner is tp else latent_all.at[at]
            return send(src, latent_all.at[at], lat_s.at[i], lat_r.at[i], "tp", target)

        to_right = pass_on(tp, 0, right, 0)
        to_left = pass_on(tp, half, left, 1)
        moves = [pass_on(tp, half, right, 2), pass_on(tp, 0, left, 3)]
    else:
        moves = [
            send(latent, latent_all.at[mine], lat_s.at[d], lat_r.at[d], "tp", p)
            for d, p in enumerate(tp_peers)
        ]
    for copy in first:
        copy.wait()
    summed = part[...]
    for d in range(tp_n - 1):
        summed += tp_box[d]
    middle[...] = summed
    second = [
        send(middle, sp_box.at[d], sps.at[d], spr.at[d], "sp", p) for d, p in enumerate(sp_peers)
    ]
    for copy in second:
        copy.wait()
    summed = middle[...]
    for d in range(sp_n - 1):
        summed += sp_box[d]
    middle[...] = summed
    mod[...] = jnp.zeros_like(mod)
    for c in range(model // LANES):
        mod[0:5, c * LANES : (c + 1) * LANES] = middle[5 * c : 5 * c + 5, :]
    for copy in halos:
        copy.wait()
    copy_lat.wait()
    copy_ctx.wait()
    if tp_n == 4:
        to_right.wait()
        moves.append(pass_on(left, 0, right, 4))
        to_left.wait()
        moves.append(pass_on(right, half, left, 5))

    modulate_into(context_ext, hidden_c, mod.at[1:2, :], mod.at[3:4, :])

    def taps_at(ref, start):
        return ref[:, pl.ds(pl.multiple_of(start, piece), piece)]

    place = lax.broadcasted_iota(jnp.int32, (ext, piece), 0)
    live = ((place >= HALO) | (sp > 0)) & ((place < HALO + ctx_rows) | (sp < sp_n - 1))

    def latent_part(weight, taps, total, out):
        for c in range(0, total, piece):
            pre = jnp.dot(hidden[...], weight[:, c : c + piece], preferred_element_type=F32)
            pre = pre.astype(BF16)
            if taps is None:
                out[:, c : c + piece] = pre
            else:
                kernel = taps_at(taps, tp * total + c)
                out[:, c : c + piece] = conv_silu(pre.astype(F32), kernel, ROW)

    def context_part(weight, taps, total, out):
        for c in range(0, total, piece):
            pre = jnp.dot(hidden_c[...], weight[:, c : c + piece], preferred_element_type=F32)
            pre = jnp.where(live, pre.astype(BF16).astype(F32), 0.0)
            done = conv_silu(pre, taps_at(taps, tp * total + c), ext)
            out[:, c : c + piece] = done[HALO : HALO + ctx_rows]

    pick_i = lax.broadcasted_iota(jnp.int32, (rates.shape[1], LANES), 0)
    pick_l = lax.broadcasted_iota(jnp.int32, (rates.shape[1], LANES), 1)
    pick = (pick_i == tp * heads + lax.rem(pick_l, heads)).astype(F32)
    chosen = jnp.dot(rates[...], pick, precision=FINEST, preferred_element_type=F32)
    lane_at = lax.broadcasted_iota(jnp.int32, (1, LANES), 1)
    rate = jnp.where(
        lane_at < heads, chosen[0:1, :], jnp.where(lane_at < 2 * heads, chosen[1:2, :], 0.0))
    loads[0].wait()
    loads[1].wait()
    context_part(value_p, value_t, width, ctx_v)
    context_part(write_p, write_t, keys, ctx_w)
    raw_c = jnp.dot(hidden_c[...], step_p[...], preferred_element_type=F32).astype(BF16)
    step_c = softplus(raw_c.astype(F32))[HALO : HALO + ctx_rows]
    decay_c = -rate * step_c
    total_c = jnp.sum(decay_c, axis=0, keepdims=True)
    weight_c = jnp.exp(total_c - running(decay_c, heads)) * step_c
    found = partial_states(ctx_v[...], ctx_w[...], weight_c, heads, per_group)
    for h in range(heads):
        at = slice(h * HEAD, (h + 1) * HEAD)
        c_states[0, at, :] = found[h][:, 0:STATE].astype(BF16)
        c_states[1, at, :] = found[h][:, STATE : 2 * STATE].astype(BF16)
    c_tots[...] = lane_to_rows(total_c, 2 * heads)

    share = width // sp_n

    def share_of(p):
        return pl.ds(pl.multiple_of(p * share, share), share)

    gathers = []
    for d, p in enumerate(sp_peers):
        gathers.append(send(c_tots, c_tot_box.at[sp], s2.at[d], r2.at[d], "sp", p))
        gathers.append(
            send(c_states.at[:, share_of(p), :], c_box.at[sp], s1.at[d], r1.at[d], "sp", p))
    c_box[sp] = c_states[:, share_of(sp), :]
    c_tot_box[sp] = c_tots[...]

    for copy in moves:
        copy.wait()
    modulate_into(latent_all, hidden, mod.at[0:1, :], mod.at[2:3, :])

    for copy in gathers:
        copy.wait()
    head_at = (sp * share) // HEAD
    each = min(HEAD, share)

    def factor(j, base):
        found = [
            jnp.broadcast_to(
                jnp.exp(c_tot_box[j, pl.ds(base + head_at + q, 1), :]), (each, STATE))
            for q in range(max(1, share // HEAD))
        ]
        return found[0] if len(found) == 1 else jnp.concatenate(found, axis=0)

    forward = jnp.zeros((share, STATE), F32)
    for j in range(sp_n):
        forward = factor(j, 0) * forward + c_box[j, 0].astype(F32)
    backward = jnp.zeros((share, STATE), F32)
    for j in range(sp_n - 1, -1, -1):
        backward = factor(j, heads) * backward + c_box[j, 1].astype(F32)
    c_out[0] = forward.astype(BF16)
    c_out[1] = backward.astype(BF16)
    back = [
        send(c_out, ctx_o.at[:, share_of(sp), :], s3.at[d], r3.at[d], "sp", p)
        for d, p in enumerate(sp_peers)
    ]
    ctx_o[:, share_of(sp), :] = c_out[...]

    latent_part(value_p, value_t, width, values_o)
    latent_part(write_p, write_t, keys, writes_o)
    loads[2].wait()
    loads[3].wait()
    latent_part(gate_p, None, width, gate_o)
    latent_part(read_p, read_t, keys, reads_o)
    raw = jnp.dot(hidden[...], step_p[...], preferred_element_type=F32).astype(BF16)
    pace = pacing[:, pl.ds(pl.multiple_of(sp * tokens, tokens), tokens)]
    pace = jnp.broadcast_to(pace, (LANES, tokens)).T
    step_o[...] = softplus(raw.astype(F32)) * pace
    drops = []
    for k in range(blocks):
        at = slice(k * BLOCK, (k + 1) * BLOCK)
        step = step_o[at, :]
        decay = -rate * step
        cumul = running(decay, heads)
        total = jnp.sum(decay, axis=0, keepdims=True)
        cumul_o[at, :] = cumul
        weight = jnp.exp(total - cumul) * step
        drops.append(jnp.exp(total))
        found = partial_states(values_o[at, :], writes_o[at, :], weight, heads, per_group)
        for h in range(heads):
            inc_o[k, h * HEAD : (h + 1) * HEAD, :] = found[h]
    for h in range(heads):
        at = slice(h * HEAD, (h + 1) * HEAD)
        forward = inc_o[0, at, 0:STATE]
        for k in range(1, blocks):
            forward = drops[k][:, h : h + 1] * forward + inc_o[k, at, 0:STATE]
        backward = inc_o[blocks - 1, at, STATE : 2 * STATE]
        for k in range(blocks - 2, -1, -1):
            backward = (
                drops[k][:, heads + h : heads + h + 1] * backward
                + inc_o[k, at, STATE : 2 * STATE])
        ends_o[0, at, :] = forward
        ends_o[1, at, :] = backward
    for copy in back:
        copy.wait()


def sweep_kernel(
    sp_n, heads, per_group,
    values, gate, writes, reads, step, cumul, inc, ends, ctx, gain,
    inner,
    starts, outgoing, state_f, state_b, joined, ss, rs,
):
    sp, tp = lax.axis_index("sp"), lax.axis_index("tp")
    tokens, width = values.shape
    blocks = tokens // BLOCK
    span = per_group * HEAD
    groups = heads // per_group
    after, before = lax.rem(sp + 1, sp_n), lax.rem(sp + sp_n - 1, sp_n)
    lane = lax.broadcasted_iota(jnp.int32, (1, LANES), 1)
    totals = [
        jnp.where(
            lane < heads,
            cumul[(k + 1) * BLOCK - 1 : (k + 1) * BLOCK, :],
            cumul[k * BLOCK : k * BLOCK + 1, :])
        for k in range(blocks)
    ]
    drops = [jnp.exp(t) for t in totals]
    grand = totals[0]
    for t in totals[1:]:
        grand = grand + t
    grand = jnp.exp(grand)
    chunk = 2 * HEAD
    chunks = width // chunk

    def link(way, c):
        at = pl.ds(c * chunk, chunk)
        return pltpu.make_async_remote_copy(
            src_ref=outgoing.at[way, at],
            dst_ref=starts.at[way, at],
            send_sem=ss.at[way * chunks + c],
            recv_sem=rs.at[way * chunks + c],
            device_id={"sp": before if way else after},
            device_id_type=MESH,
        )

    def chain(way):
        enters = sp == (sp_n - 1 if way else 0)
        leaves = sp == (0 if way else sp_n - 1)

        @pl.when(enters)
        def _():
            starts[way] = ctx[way]

        for c in range(chunks):
            @pl.when(jnp.logical_not(enters))
            def _():
                link(way, c).wait_recv()

            @pl.when(jnp.logical_not(leaves))
            def _():
                for q in range(chunk // HEAD):
                    h = c * (chunk // HEAD) + q
                    at = slice(h * HEAD, (h + 1) * HEAD)
                    j = way * heads + h
                    outgoing[way, at, :] = (
                        grand[:, j : j + 1] * starts[way, at, :].astype(F32) + ends[way, at, :]
                    ).astype(BF16)
                link(way, c).start()

    at_row = lax.broadcasted_iota(jnp.int32, (BLOCK, BLOCK), 0)
    by_row = lax.broadcasted_iota(jnp.int32, (BLOCK, BLOCK), 1)
    past, diagonal = by_row <= at_row, by_row == at_row
    contract = (((1,), (1,)), ((), ()))

    def local_block(k):
        rows = slice(k * BLOCK, (k + 1) * BLOCK)
        c = cumul[rows, :]
        c_turned, s_turned = c.T, step[rows, :].T
        for g in range(groups):
            keys = slice(g * STATE, (g + 1) * STATE)
            affinity = lax.dot_general(
                reads[rows, keys], writes[rows, keys], contract, preferred_element_type=F32)
            for r in range(per_group):
                h = g * per_group + r
                b = heads + h
                head = slice(h * HEAD, (h + 1) * HEAD)
                exponent = jnp.where(
                    past,
                    c[:, h : h + 1] - c_turned[h : h + 1, :],
                    c[:, b : b + 1] - c_turned[b : b + 1, :])
                fs, bs = s_turned[h : h + 1, :], s_turned[b : b + 1, :]
                steps = jnp.where(past, fs, bs) + jnp.where(diagonal, bs, 0.0)
                mixing = (affinity * jnp.exp(exponent) * steps).astype(BF16)
                joined[rows, head] = jnp.dot(
                    mixing, values[rows, head], preferred_element_type=F32)

    for slot in range(blocks):
        last = slot == blocks - 1
        for way in range(2):
            turn = (sp_n - 1 - sp) if way else sp
            pl.when(turn >= slot if last else turn == slot)(functools.partial(chain, way))
        local_block(slot)

    for way in range(2):
        @pl.when(sp != (0 if way else sp_n - 1))
        def _():
            for c in range(chunks):
                link(way, c).wait_send()

    for h in range(heads):
        rows = slice(h * HEAD, (h + 1) * HEAD)
        forward = starts[0, rows, :].astype(F32)
        for k in range(blocks):
            state_f[k, rows, :] = forward.astype(BF16)
            forward = drops[k][:, h : h + 1] * forward + inc[k, rows, 0:STATE]
        backward = starts[1, rows, :].astype(F32)
        for k in range(blocks - 1, -1, -1):
            state_b[k, rows, :] = backward.astype(BF16)
            backward = (
                drops[k][:, heads + h : heads + h + 1] * backward
                + inc[k, rows, STATE : 2 * STATE])

    def carried_block(k, carry):
        rows = pl.ds(pl.multiple_of(k * BLOCK, BLOCK), BLOCK)
        grown = jnp.exp(cumul[rows, :])
        for g in range(groups):
            read = reads[rows, g * STATE : (g + 1) * STATE].astype(F32)
            for r in range(per_group):
                h = g * per_group + r
                b = heads + h
                head = slice(h * HEAD, (h + 1) * HEAD)
                left = jnp.concatenate(
                    [(read * grown[:, h : h + 1]).astype(BF16),
                     (read * grown[:, b : b + 1]).astype(BF16)], axis=1)
                right = jnp.concatenate([state_f[k, head, :], state_b[k, head, :]], axis=1)
                joined[rows, head] += lax.dot_general(
                    left, right, contract, preferred_element_type=F32)
            lanes = slice(g * span, (g + 1) * span)
            gated = joined[rows, lanes] * silu(gate[rows, lanes].astype(F32))
            scale = lax.rsqrt(jnp.mean(gated * gated, -1, keepdims=True) + GATED_FLOOR)
            start = pl.multiple_of(tp * width + g * span, span)
            inner[rows, lanes] = (gated * scale * gain[:, pl.ds(start, span)]).astype(BF16)
        return carry

    lax.fori_loop(0, blocks, carried_block, 0)


def finish_kernel(tp_n, inner, out_p, total_o, mixed, early, relay, box, ss, rs):
    tp = lax.axis_index("tp")
    peers = others("tp", tp_n)
    rows, model = total_o.shape

    def product(owner):
        at = pl.ds(pl.multiple_of(owner * rows, rows), rows)
        for c in range(0, model, 512):
            mixed[at, c : c + 512] = jnp.dot(
                inner[at, :], out_p[:, c : c + 512], preferred_element_type=F32).astype(BF16)

    def rows_at(p, count, start=0):
        return pl.ds(pl.multiple_of(p * rows + start, count), count)

    if tp_n == 4:
        half = rows // 2
        low, high = pl.ds(0, half), pl.ds(half, half)
        right, left, opposite = ring_of(tp, tp_n)
        product(opposite)
        far = [
            send(mixed.at[rows_at(opposite, half)], early.at[0], ss.at[0], rs.at[0], "tp", right),
            send(mixed.at[rows_at(opposite, half, half)], early.at[1],
                 ss.at[1], rs.at[1], "tp", left),
        ]
        product(right)
        copies = [send(mixed.at[rows_at(right, half, half)], box.at[0, high],
                       ss.at[2], rs.at[2], "tp", right)]
        product(left)
        copies.append(send(mixed.at[rows_at(left, half)], box.at[1, low],
                           ss.at[3], rs.at[3], "tp", left))
        product(tp)
        for way, (owner, start, lands) in enumerate([(right, 0, low), (left, half, high)]):
            far[way].wait()
            relay[way] = (
                mixed[rows_at(owner, half, start), :].astype(F32) + early[way].astype(F32)
            ).astype(BF16)
            copies.append(send(relay.at[way], box.at[way, lands],
                               ss.at[4 + way], rs.at[4 + way], "tp", owner))
        landed = 2
    else:
        for p in peers + [tp]:
            product(p)
        copies = [
            send(mixed.at[rows_at(p, rows)], box.at[d], ss.at[d], rs.at[d], "tp", p)
            for d, p in enumerate(peers)
        ]
        landed = tp_n - 1
    for copy in copies:
        copy.wait()
    tile_rows = 16

    def tile(i, carry):
        at = pl.ds(pl.multiple_of(i * tile_rows, tile_rows), tile_rows)
        own = pl.ds(pl.multiple_of(tp * rows + i * tile_rows, tile_rows), tile_rows)
        total = mixed[own, :].astype(F32)
        for d in range(landed):
            total += box[d, at, :].astype(F32)
        total_o[at, :] = total.astype(BF16)
        return carry

    lax.fori_loop(0, rows // tile_rows, tile, 0)


def whole_kernel(sp_n, tp_n, heads, per_group, *refs):
    front_in, (gain, out_h) = refs[:16], refs[16:18]
    total_o, gate_row_o = refs[18:20]
    made, refs = refs[20:30], refs[30:]
    front, refs = refs[:FRONT], refs[FRONT:]
    sweep, refs = refs[:7], refs[7:]
    inner, out_p, out_sem = refs[:3]
    load = pltpu.make_async_copy(out_h, out_p, out_sem.at[0])
    load.start()
    front_kernel(sp_n, tp_n, heads, per_group, *front_in, *made, *front)
    values, gate, writes, reads, step, cumul, inc, ends, ctx, mod = made
    gate_row_o[...] = mod[4:5, :]
    sweep_kernel(sp_n, heads, per_group, *made[:9], gain, inner, *sweep)
    load.wait()
    finish_kernel(tp_n, inner, out_p, total_o, *refs[3:])


def shape(dims, kind):
    return jax.ShapeDtypeStruct(dims, kind)


def call(body, outs, specs, scratch, collective, limit=60 << 20):
    params = dict(vmem_limit_bytes=limit, collective_id=collective, has_side_effects=True)
    single = not isinstance(outs, (list, tuple))
    return pl.pallas_call(
        body,
        out_shape=outs,
        in_specs=specs,
        out_specs=vmem() if single else [vmem()] * len(outs),
        scratch_shapes=scratch,
        compiler_params=pltpu.CompilerParams(**params),
    )


def dma(count):
    return pltpu.SemaphoreType.DMA((count,))


def per_device(
    sp_n, tp_n,
    latent, condition, context, context_cond, shift_matrix, scale_matrix, gate_matrix,
    value_proj, gate_proj, write_proj, read_proj, step_proj, decay_rate, pacing,
    value_taps, write_taps, read_taps, norm_gain, out_proj,
):
    sp, tp = lax.axis_index("sp"), lax.axis_index("tp")
    rows, model = latent.shape[1:]
    ctx_rows = context.shape[1]
    tokens = rows * tp_n
    width, keys = value_proj.shape[1], write_proj.shape[1]
    heads = width // HEAD
    per_group = heads // (keys // STATE)
    blocks = tokens // BLOCK
    row_share = shift_matrix.shape[0]

    start = (sp * tp_n + tp) * row_share
    own_row = lax.dynamic_slice_in_dim(condition, start, row_share, 1)
    ctx_row = lax.dynamic_slice_in_dim(context_cond, start, row_share, 0)[None]
    at = lax.broadcasted_iota(jnp.int32, (48, row_share), 0)
    is_own = (at == 0) | (at == 18) | (at == 36)
    is_ctx = (at == 1) | (at == 19)
    act = jnp.where(is_own, own_row, jnp.where(is_ctx, ctx_row, 0.0))
    act = jax.nn.silu(act).astype(BF16)
    step_cols = lax.dynamic_slice_in_dim(step_proj, tp * heads, heads, 2)
    step_cols = jnp.pad(step_cols.reshape(model, 2 * heads), ((0, 0), (0, LANES - 2 * heads)))
    held = pl.BlockSpec(memory_space=pl.ANY)
    ext = ctx_rows + 2 * HALO
    share = width // sp_n
    packed = 5 * model // LANES
    pieces = 2 * (width // (2 * HEAD))
    made = [
        pltpu.VMEM((tokens, width), BF16), pltpu.VMEM((tokens, width), BF16),
        pltpu.VMEM((tokens, keys), BF16), pltpu.VMEM((tokens, keys), BF16),
        pltpu.VMEM((tokens, LANES), F32), pltpu.VMEM((tokens, LANES), F32),
        pltpu.VMEM((blocks, width, 2 * STATE), F32), pltpu.VMEM((2, width, STATE), F32),
        pltpu.VMEM((2, width, STATE), BF16), pltpu.VMEM((8, model), F32),
    ]
    front = [
        pltpu.VMEM((model, width), BF16), pltpu.VMEM((model, width), BF16),
        pltpu.VMEM((model, keys), BF16), pltpu.VMEM((model, keys), BF16),
        pltpu.VMEM((tokens, model), BF16), pltpu.VMEM((ext, model), BF16),
        pltpu.VMEM((packed, LANES), F32), pltpu.VMEM((tp_n - 1, packed, LANES), F32),
        pltpu.VMEM((packed, LANES), F32), pltpu.VMEM((sp_n - 1, packed, LANES), F32),
        pltpu.VMEM((tokens, model), BF16), pltpu.VMEM((ext, model), BF16),
        pltpu.VMEM((ctx_rows, width), BF16), pltpu.VMEM((ctx_rows, keys), BF16),
        pltpu.VMEM((2, width, STATE), BF16), pltpu.VMEM((2 * heads, LANES), F32),
        pltpu.VMEM((sp_n, 2, share, STATE), BF16), pltpu.VMEM((sp_n, 2 * heads, LANES), F32),
        pltpu.VMEM((2, share, STATE), BF16),
        dma(6), dma(max(6, tp_n)), dma(max(6, tp_n)), dma(tp_n), dma(tp_n),
        dma(sp_n), dma(sp_n), dma(2), dma(2),
        dma(sp_n), dma(sp_n), dma(sp_n), dma(sp_n), dma(sp_n), dma(sp_n),
    ]
    assert len(front) == FRONT
    sweep = [
        pltpu.VMEM((2, width, STATE), BF16), pltpu.VMEM((2, width, STATE), BF16),
        pltpu.VMEM((blocks, width, STATE), BF16), pltpu.VMEM((blocks, width, STATE), BF16),
        pltpu.VMEM((tokens, width), F32), dma(pieces), dma(pieces),
    ]
    finish = [
        pltpu.VMEM((tokens, width), BF16), pltpu.VMEM((width, model), BF16), dma(1),
        pltpu.VMEM((tokens, model), BF16), pltpu.VMEM((2, rows // 2, model), BF16),
        pltpu.VMEM((2, rows // 2, model), BF16), pltpu.VMEM((tp_n - 1, rows, model), BF16),
        dma(6), dma(6),
    ]
    total, gate_row = call(
        functools.partial(whole_kernel, sp_n, tp_n, heads, per_group),
        [shape((rows, model), BF16), shape((1, model), F32)],
        [vmem()] * 6 + [held] * 4 + [vmem()] * 7 + [held],
        made + front + sweep + finish,
        0,
    )(act, shift_matrix, scale_matrix, gate_matrix, latent[0], context[0],
      value_proj, gate_proj, write_proj, read_proj, step_cols,
      decay_rate, pacing, value_taps, write_taps, read_taps, norm_gain[None], out_proj)
    updated = latent[0].astype(F32) + gate_row * lax.optimization_barrier(total).astype(F32)
    return updated.astype(BF16)[None]


def solution(mesh):
    placed = (
        P("dp", ("sp", "tp"), None),
        P("dp", None),
        P("dp", "sp", None),
        P(),
        P(("sp", "tp"), None),
        P(("sp", "tp"), None),
        P(("sp", "tp"), None),
        P(None, "tp"),
        P(None, "tp"),
        P(None, "tp"),
        P(None, "tp"),
        P(),
        P(),
        P("dp", None),
        P(),
        P(),
        P(),
        P(),
        P("tp", None),
    )
    return jax.shard_map(
        functools.partial(per_device, mesh.shape["sp"], mesh.shape["tp"]),
        mesh=mesh,
        in_specs=placed,
        out_specs=P("dp", ("sp", "tp"), None),
        check_vma=False,
    )
```
